512 devices in a mesh: ep: 32 (over z, core), tp: 16 (over y, x).
Axes of the slice: x: 4, y: 4, z: 16, core: 2. Of those that a mesh axis runs over, the one named last changes fastest.
Arguments:
- query_rows: bfloat16 [24576, 1024], P('ep', 'tp'), may hold values from -600 to 600
- key_rows: bfloat16 [24576, 1024], P('ep', 'tp'), may hold values from -6 to 6
- value_rows: bfloat16 [24576, 1024], P('ep', 'tp'), may hold values from -6 to 6
- cum_gate: float32 [16, 24576], P('tp'), may hold values from -2458 to 0, as said below
- out_weight: bfloat16 [1024, 2048], P(None, 'tp'), may hold values from -0.1875 to 0.1875
- moe_input: bfloat16 [6144, 2048], P('ep'), may hold values from -6 to 6
- moe_gain: float32 [2048], replicated, may hold values from 0.1 to 1.9
- routes: int32 [6144, 3], P('ep'), may hold values from 0 to 127, all different within a row; in each aligned block of 192 rows (0 to 191, 192 to 383, ...) at most 9 rows name the same one
- route_weight: float32 [6144, 3], P('ep'), may hold values from 0.2 to 1.5
- expert_gate: bfloat16 [128, 2048, 512], P('ep', None, 'tp'), may hold values from -0.125 to 0.125
- expert_up: bfloat16 [128, 2048, 512], P('ep', None, 'tp'), may hold values from -0.125 to 0.125
- expert_down: bfloat16 [128, 512, 2048], P('ep', None, 'tp'), may hold values from -0.25 to 0.25
- shared_gate: bfloat16 [2048, 512], P(None, 'tp'), may hold values from -0.125 to 0.125
- shared_up: bfloat16 [2048, 512], P(None, 'tp'), may hold values from -0.125 to 0.125
- shared_down: bfloat16 [512, 2048], P(None, 'tp'), may hold values from -0.25 to 0.25
Outputs:
- mixer_out: bfloat16 [24576, 2048], P('ep', 'tp')
- moe_out: bfloat16 [6144, 2048], P('ep', 'tp')
The draws below stay inside these ranges and needn't reach their ends.
Inputs may be any that keep to these rules, and one draw needn't show every extreme that they name: Non-increasing along positions: cum_gate[h, t] is the sum of the log forget gates of head h over positions 0 to t. `routes`: the 3 experts of a token differ. In each aligned block of 192 tokens no expert is named by more than 9 tokens, a bound that some block reaches.
All inputs are finite; a program needn't handle non-finite values.
Results may differ from the reference program's by a relative error of at most 0.0068.
Values may be sent and summed in bfloat16 or wider, within the bound.
A program may use at most 64 MiB of HBM per device.

```python
import math
import jax
import jax.numpy as jnp
import numpy as np
from jax import lax

D = 2048
HEADS = 16
HEAD = 64
FF = 512
FS = 512
EXPERTS = 128
TOP = 3
SEQ_DEV = 768
LENGTH = 24576
MOE_DEV = 192
TOKENS_MOE = 6144
CAP = 9
N_EP = 32


def draw_query_rows(key, part):
    base_key = jax.random.fold_in(key, 7)
    key_normal = jax.random.fold_in(base_key, 0)
    drawn = jnp.clip(jax.random.normal(key_normal, (LENGTH, HEADS * HEAD), jnp.float32), -6.0, 6.0)
    return drawn.astype(jnp.bfloat16)


def draw_cum_gate(key, part):
    base_key = jax.random.fold_in(key, 13)
    key_heads, key_steps, key_blocks = jax.random.split(base_key, 3)
    head_order = jax.random.permutation(key_heads, HEADS)
    fast_count = HEADS // 2
    decay_rates = jnp.where(head_order < fast_count, 1.0 / 40.0, 1.0 / LENGTH).astype(jnp.float32)
    low = jnp.log(0.5)
    high = jnp.log(2.0)
    step_factors = jnp.exp(jax.random.uniform(key_steps, (HEADS, LENGTH), jnp.float32, low, high))
    block_factors = jnp.exp(jax.random.uniform(key_blocks, (HEADS, LENGTH // SEQ_DEV), jnp.float32, low, high))
    block_factors = jnp.repeat(block_factors, SEQ_DEV, axis=1)
    log_gates = -decay_rates[:, None] * step_factors * block_factors
    return jnp.cumsum(log_gates, axis=1).astype(jnp.float32)


def levels(rng, shape, cuts, least, high):
    def one(axis_at, shards_of):
        draws = jax.random.uniform(jax.random.fold_in(jax.random.fold_in(rng, 6), axis_at), (shards_of,), jnp.float32, least / len(cuts), high / len(cuts))
        return jnp.repeat(jnp.exp(draws), shape[axis_at] // shards_of).reshape((-1,) + (1,) * (len(shape) - axis_at - 1))

    loudness = one(*cuts[0])
    for cut in cuts[1:]:
        loudness = loudness * one(*cut)
    return loudness


def deal_out(rng, own, number, rows, amount, top, limit, slope):
    order = jax.random.permutation(rng, amount)
    heavy_load, common = load_shares(amount, rows * top, limit, slope, True), load_shares(amount, rows * top, limit, slope, False)
    places = jnp.arange(amount)

    def named(tallies, turn):
        used = int((tallies > 0).sum())
        fixed = max(1, used // 4)
        shifted = fixed + (places - fixed + turn * (used - fixed)) % max(1, amount - fixed)
        return jnp.zeros((amount,), jnp.int32).at[order[jnp.where(places < fixed, places, shifted)]].set(jnp.asarray(tallies, jnp.int32))

    tallies = jnp.where(number % 4 == 0, named(heavy_load, number // 4), named(common, number - number // 4 - 1))
    mixed = jax.random.permutation(jax.random.fold_in(own, 3), amount)
    donor, receiver = mixed[0:amount // 2 * 2:2], mixed[1:amount // 2 * 2:2]
    margin = jnp.minimum(tallies[donor] - 1, limit - tallies[receiver]) // 2
    margin = jnp.where((donor == order[0]) | (receiver == order[0]) | (tallies[receiver] == 0), 0, jnp.maximum(margin, 0))
    shifted = jax.random.randint(jax.random.fold_in(own, 4), (amount // 2,), 0, 1 << 20) % (margin + 1)
    tallies = tallies.at[donor].add(-shifted).at[receiver].add(shifted)
    members = jnp.searchsorted(jnp.cumsum(tallies), jnp.arange(rows * top), side="right").astype(jnp.int32)
    listing = members.reshape(top, rows).T
    listing = listing[jax.random.permutation(jax.random.fold_in(own, 1), rows)]
    turn = jax.random.randint(jax.random.fold_in(own, 2), (rows, 1), 0, top)
    return jnp.take_along_axis(listing, (jnp.arange(top)[None, :] + turn) % top, axis=1)


def load_shares(amount, total, reach, skew, full):
    portions = [(1 << 20) // math.isqrt(standing ** skew) + 1 for standing in range(1, amount + 1)]
    largest = reach if full else min(reach, max(-(-total // amount), total * portions[0] // sum(portions)))
    least = 1 if total - largest >= amount - 1 else 0
    holding, rest = [largest] + [least] * (amount - 1), total - largest - least * (amount - 1)
    while rest > 0:
        free = [i for i in range(1, amount) if holding[i] < largest] or [i for i in range(1, amount) if holding[i] < reach]
        pool, left = sum([portions[i] for i in free]), rest
        for i in free:
            more = min(reach - holding[i], max(1, left * portions[i] // pool), rest)
            holding[i] = holding[i] + more
            rest = rest - more
    return np.array(holding)


def bell_draw(stream_key, shape, deviation, limit, cuts=(), kind=jnp.bfloat16):
    array = jax.random.normal(stream_key, shape, jnp.float32) * deviation
    if len(cuts) > 0:
        array = levels(stream_key, shape, cuts, -0.22, 0.18) * array
    return jnp.clip(array, min=-limit, max=limit).astype(kind)


def setup_inputs(seed: int = 0) -> dict:
    keys = jax.random.split(jax.random.key(seed), 16)
    query_rows = draw_query_rows(jax.random.fold_in(keys[15], 71), 0)
    key_rows = bell_draw(keys[1], (LENGTH, HEADS * HEAD), 1.0, 6.0, ((0, 32), (1, 16)))
    value_rows = bell_draw(keys[2], (LENGTH, HEADS * HEAD), 1.0, 6.0, ((0, 32), (1, 16)))
    cum_gate = draw_cum_gate(jax.random.fold_in(keys[15], 71), 0)
    out_weight = bell_draw(keys[4], (HEADS * HEAD, D), (HEADS * HEAD) ** -0.5, 0.1875, ((1, 16),))
    moe_input = bell_draw(keys[5], (TOKENS_MOE, D), 1.0, 6.0, ((0, 32),))
    moe_gain = jnp.clip(1.0 + 0.18 * jax.random.normal(keys[6], (D,), jnp.float32), 0.1, 1.9)
    routes_keys = jax.random.split(jax.random.fold_in(keys[7], 1), TOKENS_MOE // MOE_DEV)
    routes_turns = jax.random.permutation(jax.random.fold_in(keys[7], 3), TOKENS_MOE // MOE_DEV)
    routes = jax.vmap(lambda own, number: deal_out(jax.random.fold_in(keys[7], 2), own, number, MOE_DEV, EXPERTS, TOP, CAP, 2))(routes_keys, routes_turns).reshape((TOKENS_MOE, TOP))
    route_weight = jnp.clip(jnp.exp(math.log(1.5) - 2.014903 * jax.random.uniform(keys[8], (TOKENS_MOE, TOP), jnp.float32) ** levels(keys[8], (TOKENS_MOE, TOP), ((0, 32),), -0.2, 0.2)), 0.2, 1.5)
    expert_gate = bell_draw(keys[9], (EXPERTS, D, FF), D ** -0.5, 0.125, ((0, 32), (2, 16)))
    expert_up = bell_draw(keys[10], (EXPERTS, D, FF), D ** -0.5, 0.125, ((0, 32), (2, 16)))
    expert_down = bell_draw(keys[11], (EXPERTS, FF, D), FF ** -0.5, 0.25, ((0, 32), (2, 16)))
    shared_gate = bell_draw(keys[12], (D, FS), D ** -0.5, 0.125, ((1, 16),))
    shared_up = bell_draw(keys[13], (D, FS), D ** -0.5, 0.125, ((1, 16),))
    shared_down = bell_draw(keys[14], (FS, D), FS ** -0.5, 0.25, ((1, 16),))
    return {"query_rows": query_rows, "key_rows": key_rows, "value_rows": value_rows, "cum_gate": cum_gate, "out_weight": out_weight, "moe_input": moe_input, "moe_gain": moe_gain, "routes": routes, "route_weight": route_weight, "expert_gate": expert_gate, "expert_up": expert_up, "expert_down": expert_down, "shared_gate": shared_gate, "shared_up": shared_up, "shared_down": shared_down}


neg_fill = -1e+30
norm_eps = 1e-06

def attention_heads(query_rows, key_rows, value_rows, cum_gate):
    query_span = 128 if LENGTH % 128 == 0 else LENGTH
    query_heads = query_rows.reshape(LENGTH, HEADS, HEAD)
    key_heads = key_rows.reshape(LENGTH, HEADS, HEAD).astype(jnp.float32)
    value_heads = value_rows.reshape(LENGTH, HEADS, HEAD).astype(jnp.float32)
    key_pos = jnp.arange(LENGTH, dtype=jnp.int32)
    scale = HEAD ** (-0.5)

    def one_block(block_index):
        start = (block_index * query_span).astype(jnp.int32)
        query_block = lax.dynamic_slice_in_dim(query_heads, start, query_span, 0).astype(jnp.float32)
        query_gate = lax.dynamic_slice_in_dim(cum_gate, start, query_span, 1)
        scores = jnp.einsum('qhd,khd->hqk', query_block, key_heads) * scale
        scores = scores + query_gate[:, :, None] - cum_gate[:, None, :]
        query_pos = start + jnp.arange(query_span, dtype=jnp.int32)
        causal = key_pos[None, :] <= query_pos[:, None]
        scores = jnp.where(causal[None], scores, neg_fill)
        row_max = lax.optimization_barrier(jnp.max(scores, axis=2, keepdims=True))
        expon = jnp.where(causal[None], jnp.exp(scores - row_max), 0.0)
        denom = lax.optimization_barrier(jnp.sum(expon, axis=2))
        probs = lax.optimization_barrier(expon.astype(jnp.bfloat16)).astype(jnp.float32)
        summed = jnp.einsum('hqk,khd->qhd', probs, value_heads)
        result = summed / jnp.transpose(denom)[:, :, None]
        return result.astype(jnp.bfloat16).reshape(query_span, HEADS * HEAD)
    blocks = lax.map(one_block, jnp.arange(LENGTH // query_span, dtype=jnp.int32))
    return blocks.reshape(LENGTH, HEADS * HEAD)

def experts_branch(moe_input, moe_gain, routes, route_weight, expert_gate, expert_up, expert_down, shared_gate, shared_up, shared_down):
    moe_rows = moe_input.astype(jnp.float32)
    normed = (moe_rows * lax.rsqrt(lax.optimization_barrier(jnp.mean(moe_rows * moe_rows, axis=1, keepdims=True)) + norm_eps) * moe_gain).astype(jnp.bfloat16)
    pair_count = TOKENS_MOE * TOP
    flat_routes = routes.reshape(-1).astype(jnp.int32)
    one_hot = (flat_routes[:, None] == jnp.arange(EXPERTS, dtype=jnp.int32)[None, :]).astype(jnp.int32)
    one_hot = one_hot.reshape(N_EP, MOE_DEV * TOP, EXPERTS)
    ranks = lax.optimization_barrier(jnp.sum(jnp.cumsum(one_hot, axis=1) * one_hot, axis=2)).reshape(-1) - 1
    block_id = jnp.arange(pair_count, dtype=jnp.int32) // (MOE_DEV * TOP)
    slot_index = (flat_routes * (N_EP * CAP) + block_id * CAP + ranks).astype(jnp.int32)
    pair_token = jnp.arange(pair_count, dtype=jnp.int32) // TOP
    slot_token = jnp.full((EXPERTS * N_EP * CAP,), TOKENS_MOE, jnp.int32).at[slot_index].set(pair_token)
    padded = jnp.concatenate([normed, jnp.zeros((1, D), jnp.bfloat16)], axis=0)

    def one_expert(pieces):
        token_index, gate_w, up_w, down_w = pieces
        gathered = padded[token_index]
        gate_val = jnp.dot(gathered, gate_w, preferred_element_type=jnp.float32)
        up_val = jnp.dot(gathered, up_w, preferred_element_type=jnp.float32)
        hidden = (jax.nn.silu(gate_val) * up_val).astype(jnp.bfloat16)
        return jnp.dot(hidden, down_w, preferred_element_type=jnp.float32).astype(jnp.bfloat16)
    results = lax.map(one_expert, (slot_token.reshape(EXPERTS, N_EP * CAP), expert_gate, expert_up, expert_down))
    picked = results.reshape(EXPERTS * N_EP * CAP, D)[slot_index].astype(jnp.float32).reshape(TOKENS_MOE, TOP, D)
    routed = lax.optimization_barrier(jnp.sum(picked * route_weight[:, :, None], axis=1))
    shared_hidden = (jax.nn.silu(jnp.dot(normed, shared_gate, preferred_element_type=jnp.float32)) * jnp.dot(normed, shared_up, preferred_element_type=jnp.float32)).astype(jnp.bfloat16)
    total = routed + jnp.dot(shared_hidden, shared_down, preferred_element_type=jnp.float32)
    return total.astype(jnp.bfloat16)

def reference(query_rows, key_rows, value_rows, cum_gate, out_weight, moe_input, moe_gain, routes, route_weight, expert_gate, expert_up, expert_down, shared_gate, shared_up, shared_down):
    heads_out = attention_heads(query_rows, key_rows, value_rows, cum_gate)
    mixer_out = jnp.dot(heads_out, out_weight, preferred_element_type=jnp.float32).astype(jnp.bfloat16)
    moe_out = experts_branch(moe_input, moe_gain, routes, route_weight, expert_gate, expert_up, expert_down, shared_gate, shared_up, shared_down)
    return (mixer_out, moe_out)
```

```python
import functools
import jax
import jax.numpy as jnp
from jax import lax
from jax.experimental import pallas as pl
from jax.experimental.pallas import tpu as pltpu
from jax.sharding import PartitionSpec as P

HEAD = 64
LOG2E = 1.4426950408889634
MESH = pl.DeviceIdType.MESH


neg_fill = -1e30
norm_eps = 1e-06


def joined_along(pieces, dim):
    dims = list(pieces.shape[1:])
    dims[dim] *= pieces.shape[0]
    return jnp.moveaxis(pieces, 0, dim).reshape(dims)


def sent_to_all(array, axis):
    copies = jnp.broadcast_to(array, (lax.axis_size(axis), *array.shape))
    return lax.all_to_all(copies, axis, split_axis=0, concat_axis=0, tiled=True)


def collect(array, axis, dim):
    return joined_along(sent_to_all(array, axis), dim)


def attn_kernel(dims, qT_ref, kv_ref, cg_ref, w_ref, out_ref,
                kv, qs, acc, mx, hg, wb,
                ring_send, ring_recv, pair_send, pair_recv, head_send, head_recv):
    Z, Y, X, R, CH = dims
    NCH = R // CH
    QT = R // 256
    NU, ND = Z // 2, Z // 2 - 1
    ep = lax.axis_index("ep")
    tp = lax.axis_index("tp")
    z, core = ep // 2, ep % 2
    y, x = tp // X, tp % X
    up = (lax.rem(ep + 2, 2 * Z), tp)
    down = (lax.rem(ep + 2 * Z - 2, 2 * Z), tp)
    partner = (2 * z + 1 - core, tp)

    def x_peer(k):
        return (ep, y * X + lax.rem(x + k, X))

    def y_peer(k):
        return (ep, lax.rem(y + k, Y) * X + x)

    barrier = pltpu.get_barrier_semaphore()
    peers = [up, down, partner] + [x_peer(k) for k in range(1, X)] + [y_peer(k) for k in range(1, Y)]
    for peer in peers:
        pl.semaphore_signal(barrier, inc=1, device_id=peer, device_id_type=MESH)
    pl.semaphore_wait(barrier, len(peers))

    def copy(src, dst, ssem, rsem, dev):
        return pltpu.make_async_remote_copy(
            src_ref=src, dst_ref=dst, send_sem=ssem, recv_sem=rsem,
            device_id=dev, device_id_type=MESH)

    def first(c, slot, dev):
        return copy(kv_ref.at[:, pl.ds(c * CH, CH)], kv.at[slot, c, 0],
                    ring_send.at[slot, c], ring_recv.at[slot, c], dev)

    def first_pair(c):
        return copy(kv_ref.at[:, pl.ds(c * CH, CH)], kv.at[0, c, 1],
                    pair_send.at[0, c], pair_recv.at[0, c], partner)

    def onward(slot, c, dev):
        return copy(kv.at[slot, c, 0], kv.at[slot + 1, c, 0],
                    ring_send.at[slot + 1, c], ring_recv.at[slot + 1, c], dev)

    def to_pair(slot, c):
        return copy(kv.at[slot, c, 0], kv.at[slot, c, 1],
                    pair_send.at[slot, c], pair_recv.at[slot, c], partner)

    for c in range(NCH):
        first(c, 1, up).start()
        first(c, NU + 1, down).start()
        first_pair(c).start()

    qpad = jnp.concatenate(
        [qT_ref[...].astype(jnp.float32) * (HEAD ** -0.5), jnp.zeros((HEAD, R), jnp.float32)], axis=0)
    qs[...] = jnp.transpose(qpad).astype(jnp.bfloat16)
    mx[...] = jnp.full(mx.shape, neg_fill, jnp.float32)
    acc[...] = jnp.zeros(acc.shape, jnp.float32)
    wb[...] = jnp.zeros(wb.shape, jnp.bfloat16)

    def place(h, _):
        part = w_ref[pl.ds(pl.multiple_of(h * HEAD, HEAD), HEAD), :]
        wb[pl.ds(pl.multiple_of(h * 128, 128), HEAD), 0:128] = part
        wb[pl.ds(pl.multiple_of(h * 128 + HEAD, HEAD), HEAD), 128:256] = part
        return 0

    lax.fori_loop(0, w_ref.shape[0] // HEAD, place, 0)

    first_row = pl.multiple_of(ep * R, 128)
    base_gate = cg_ref[:, pl.ds(first_row, 128)][:, 0:1]

    def gate_of(block, c):
        at = pl.multiple_of(block * R + c * CH, 128)
        return (cg_ref[:, pl.ds(at, CH)] - base_gate) * LOG2E

    def with_ones(keys):
        row = lax.broadcasted_iota(jnp.int32, keys.shape, 0)
        return jnp.where(row < HEAD, jnp.ones_like(keys), keys)

    def update(i, parts):
        rows = slice(i * 256, (i + 1) * 256)
        q = qs[rows, :]
        logits = []
        for keys, gate, masked in parts:
            s = jnp.dot(q, keys, preferred_element_type=jnp.float32) * LOG2E - gate
            if masked:
                qi = lax.broadcasted_iota(jnp.int32, s.shape, 0)
                ki = lax.broadcasted_iota(jnp.int32, s.shape, 1)
                s = jnp.where(ki <= qi, s, neg_fill)
            logits.append(s)
        top = logits[0]
        for s in logits[1:]:
            top = jnp.maximum(top, s)
        old = mx[rows, 0:1]
        new = jnp.maximum(old, jnp.max(top, axis=1, keepdims=True))
        total = acc[rows, :] * jnp.exp2(old - new)
        for s, (keys, gate, masked) in zip(logits, parts):
            p = jnp.exp2(s - new).astype(jnp.bfloat16)
            total = total + lax.dot_general(
                p, with_ones(keys), (((1,), (1,)), ((), ())), preferred_element_type=jnp.float32)
        acc[rows, :] = total
        mx[rows, :] = jnp.broadcast_to(new, (256, 128))

    for c in range(NCH):
        keys = kv_ref[:, c * CH:(c + 1) * CH]
        for i in range(c, QT):
            update(i, [(keys, gate_of(ep, c), i == c)])

    for c in range(NCH):
        to = first_pair(c)
        to.wait_recv()

    @pl.when(core == 1)
    def _():
        for c in range(NCH):
            keys = kv[0, c, 1]
            for i in range(QT):
                update(i, [(keys, gate_of(ep - 1, c), False)])

    def issue(s, c):
        onward(s - 1, c, up).wait_recv()
        to_pair(s, c).start()

        @pl.when(s < NU)
        def _():
            onward(s, c, up).start()

        @pl.when(s <= ND)
        def _():
            onward(NU + s - 1, c, down).wait_recv()
            to_pair(NU + s, c).start()

        @pl.when(s < ND)
        def _():
            onward(NU + s, c, down).start()

    def attend(slot, c, chip):
        parts = []
        for k, block in ((0, 2 * chip + core), (1, 2 * chip + 1 - core)):
            parts.append((kv.at[slot, c, k], gate_of(block, c)))
        for i in range(QT):
            update(i, [(ref[...], gate, False) for ref, gate in parts])

    def consume(s, c):
        to_pair(s, c).wait_recv()

        @pl.when(z - s >= 0)
        def _():
            attend(s, c, z - s)

        @pl.when(s <= ND)
        def _():
            to_pair(NU + s, c).wait_recv()

            @pl.when(z + s >= Z)
            def _():
                attend(NU + s, c, z + s - Z)

    steps = NU * NCH

    def step(t, _):
        @pl.when(t < steps)
        def _():
            issue(t // NCH + 1, t % NCH)

        @pl.when(t >= 1)
        def _():
            consume((t - 1) // NCH + 1, (t - 1) % NCH)

        return 0

    lax.fori_loop(0, steps + 1, step, 0)

    quarter, half = R // 4, R // 2
    low = lax.broadcasted_iota(jnp.int32, (quarter, 128), 1) < HEAD

    def finished(at):
        a = acc[at:at + quarter, :]
        return a / pltpu.roll(a, HEAD, 1)

    for h in range(2):
        first_half = pltpu.roll(finished(h * quarter), HEAD, 1)
        second_half = finished(half + h * quarter)
        hg[h, y, x] = jnp.where(low, first_half, second_half).astype(jnp.bfloat16)

    def spread(h, phase, k):
        along_x = (h == 0) == (phase == 0)
        dev = x_peer(k) if along_x else y_peer(k)
        if phase == 0:
            ref = hg.at[h, y, x]
        elif along_x:
            ref = hg.at[h, :, x]
        else:
            ref = hg.at[h, y]
        return copy(ref, ref, head_send.at[h, phase, k], head_recv.at[h, phase, k], dev)

    def spread_in(h, phase, k):
        along_x = (h == 0) == (phase == 0)
        n = X if along_x else Y
        src_x = lax.rem(x + X - k, X)
        src_y = lax.rem(y + Y - k, Y)
        if phase == 0:
            ref = hg.at[h, y, src_x] if along_x else hg.at[h, src_y, x]
        elif along_x:
            ref = hg.at[h, :, src_x]
        else:
            ref = hg.at[h, src_y]
        return copy(ref, ref, head_send.at[h, phase, k], head_recv.at[h, phase, k], partner)

    def count(h, phase):
        return X if (h == 0) == (phase == 0) else Y

    for phase in range(2):
        for h in range(2):
            if phase == 1:
                for k in range(1, count(h, 0)):
                    spread_in(h, 0, k).wait_recv()
            for k in range(1, count(h, phase)):
                spread(h, phase, k).start()

    for h in range(2):
        for k in range(1, count(h, 1)):
            spread_in(h, 1, k).wait_recv()
        heads = X * Y
        flat = hg.at[h]
        total = jnp.zeros((quarter, 256), jnp.float32)
        for pair in range(heads // 2):
            a, b = 2 * pair, 2 * pair + 1
            lhs = jnp.concatenate([flat[a // X, a % X], flat[b // X, b % X]], axis=1)
            total = total + jnp.dot(lhs, wb[pair * 256:(pair + 1) * 256, :],
                                    preferred_element_type=jnp.float32)
        out_ref[h * quarter:(h + 1) * quarter, :] = total[:, 0:128].astype(jnp.bfloat16)
        out_ref[half + h * quarter:half + (h + 1) * quarter, :] = total[:, 128:256].astype(jnp.bfloat16)

    for c in range(NCH):
        first(c, 1, up).wait_send()
        first(c, NU + 1, down).wait_send()
        first_pair(c).wait_send()

    def drain(s, _):
        for c in range(NCH):
            to_pair(s, c).wait_send()

            @pl.when(s < NU)
            def _():
                onward(s, c, up).wait_send()

            @pl.when(s <= ND)
            def _():
                to_pair(NU + s, c).wait_send()

            @pl.when(s < ND)
            def _():
                onward(NU + s, c, down).wait_send()
        return 0

    lax.fori_loop(1, NU + 1, drain, 0)
    for phase in range(2):
        for h in range(2):
            for k in range(1, count(h, phase)):
                spread(h, phase, k).wait_send()


def attention(sizes, query_rows, key_rows, value_rows, cum_gate, out_weight):
    n_ep, Y, X = sizes
    Z = n_ep // 2
    R = query_rows.shape[0]
    CH = 256
    NU = Z // 2
    heads = X * Y
    kv = jnp.concatenate([key_rows.T, value_rows.T], axis=0)
    vm = pl.BlockSpec(memory_space=pltpu.VMEM)
    return pl.pallas_call(
        functools.partial(attn_kernel, (Z, Y, X, R, CH)),
        out_shape=jax.ShapeDtypeStruct((R, out_weight.shape[1]), jnp.bfloat16),
        in_specs=[vm] * 4,
        out_specs=vm,
        scratch_shapes=[
            pltpu.VMEM((Z, R // CH, 2, 2 * HEAD, CH), jnp.bfloat16),
            pltpu.VMEM((R, 128), jnp.bfloat16),
            pltpu.VMEM((R, 128), jnp.float32),
            pltpu.VMEM((R, 128), jnp.float32),
            pltpu.VMEM((2, Y, X, R // 4, 128), jnp.bfloat16),
            pltpu.VMEM((heads * 128, 256), jnp.bfloat16),
            pltpu.SemaphoreType.DMA((Z, R // CH)),
            pltpu.SemaphoreType.DMA((Z, R // CH)),
            pltpu.SemaphoreType.DMA((Z, R // CH)),
            pltpu.SemaphoreType.DMA((Z, R // CH)),
            pltpu.SemaphoreType.DMA((2, 2, 4)),
            pltpu.SemaphoreType.DMA((2, 2, 4)),
        ],
        compiler_params=pltpu.CompilerParams(
            collective_id=0, has_side_effects=True, vmem_limit_bytes=48 * 1024 * 1024),
    )(query_rows.T, kv, cum_gate, out_weight)


def local(
    query_rows,
    key_rows,
    value_rows,
    cum_gate,
    out_weight,
    moe_input,
    moe_gain,
    routes,
    route_weight,
    expert_gate,
    expert_up,
    expert_down,
    shared_gate,
    shared_up,
    shared_down,
):
    tp_count = lax.axis_size("tp")
    x_count = 4 if tp_count == 16 else 2
    sizes = (lax.axis_size("ep"), tp_count // x_count, x_count)
    mixer_out = attention(sizes, query_rows, key_rows, value_rows, cum_gate, out_weight)
    token_count = moe_input.shape[0]
    top_count = routes.shape[1]
    local_experts = expert_gate.shape[0]
    ep_count = lax.axis_size("ep")
    expert_count = local_experts * ep_count
    capacity = 2 * token_count * top_count // expert_count
    column_count = expert_down.shape[2]
    first_column = lax.axis_index("tp") * column_count
    moe_rows = moe_input.astype(jnp.float32)
    normed = (
        moe_rows
        * lax.rsqrt(jnp.mean(moe_rows * moe_rows, axis=1, keepdims=True) + norm_eps)
        * moe_gain
    ).astype(jnp.bfloat16)
    flat_routes = routes.reshape(-1)
    one_hot = (flat_routes[:, None] == jnp.arange(expert_count, dtype=jnp.int32)[None, :]).astype(
        jnp.int32
    )
    ranks = jnp.sum(jnp.cumsum(one_hot, axis=0) * one_hot, axis=1) - 1
    slot_index = flat_routes * capacity + ranks
    pair_token = jnp.arange(token_count * top_count, dtype=jnp.int32) // top_count
    slot_token = (
        jnp.full((expert_count * capacity,), token_count, jnp.int32).at[slot_index].set(pair_token)
    )
    padded = jnp.concatenate([normed, jnp.zeros((1, normed.shape[1]), jnp.bfloat16)], axis=0)
    outgoing = lax.dynamic_slice_in_dim(padded, first_column, column_count, 1)[slot_token]
    outgoing = outgoing.reshape(ep_count, local_experts, capacity, outgoing.shape[1])
    arrived = lax.all_to_all(outgoing, "ep", split_axis=0, concat_axis=0, tiled=True)
    arrived = lax.all_gather(arrived, "tp", axis=3, tiled=True)
    gate_val = jnp.einsum(
        "aecd,edf->aecf", arrived, expert_gate, preferred_element_type=jnp.float32
    )
    up_val = jnp.einsum("aecd,edf->aecf", arrived, expert_up, preferred_element_type=jnp.float32)
    hidden = (jax.nn.silu(gate_val) * up_val).astype(jnp.bfloat16)
    hidden = collect(hidden, "tp", 3)
    result = jnp.einsum(
        "aecf,efd->aecd", hidden, expert_down, preferred_element_type=jnp.float32
    ).astype(jnp.bfloat16)
    returned = lax.all_to_all(result, "ep", split_axis=0, concat_axis=0, tiled=True)
    picked = returned.reshape(expert_count * capacity, column_count)[slot_index]
    picked = picked.astype(jnp.float32).reshape(token_count, top_count, column_count)
    routed = jnp.sum(picked * route_weight[:, :, None], axis=1)
    shared_hidden = (
        jax.nn.silu(jnp.dot(normed, shared_gate, preferred_element_type=jnp.float32))
        * jnp.dot(normed, shared_up, preferred_element_type=jnp.float32)
    ).astype(jnp.bfloat16)
    shared_all = lax.all_gather(shared_hidden, "tp", axis=1, tiled=True)
    moe_total = routed + jnp.dot(shared_all, shared_down, preferred_element_type=jnp.float32)
    return (mixer_out, moe_total.astype(jnp.bfloat16))


def solution(mesh):
    placed = (
        P("ep", "tp"),
        P("ep", "tp"),
        P("ep", "tp"),
        P("tp", None),
        P(None, "tp"),
        P("ep", None),
        P(),
        P("ep", None),
        P("ep", None),
        P("ep", None, "tp"),
        P("ep", None, "tp"),
        P("ep", None, "tp"),
        P(None, "tp"),
        P(None, "tp"),
        P(None, "tp"),
    )
    return jax.shard_map(
        local, mesh=mesh, in_specs=placed, out_specs=(P("ep", "tp"), P("ep", "tp")), check_vma=False
    )
```

```python
import functools
import jax
import jax.numpy as jnp
from jax import lax
from jax.experimental import pallas as pl
from jax.experimental.pallas import tpu as pltpu
from jax.sharding import PartitionSpec as P

HEAD = 64
TOP = 3
LOG2E = 1.4426950408889634
MESH = pl.DeviceIdType.MESH
STOPS = (2, 7, 12, 15)
neg_fill = -1e30
norm_eps = 1e-06


def in_three(value):
    hi = value.astype(jnp.bfloat16)
    left = value - hi.astype(jnp.float32)
    mid = left.astype(jnp.bfloat16)
    low = (left - mid.astype(jnp.float32)).astype(jnp.bfloat16)
    return hi, mid, low


def step_kernel(dims, stops, *refs):
    qT_ref, kv_ref, cg_ref, w_ref = refs[0:4]
    expert_ins = refs[4:15]
    out_ref, moe_ref = refs[15:17]
    kv, qs, acc, mx, hg, wb, ring_send, ring_recv, pair_send, pair_recv, head_send, head_recv = refs[17:29]
    expert_scratch_refs = refs[29:]
    Z, Y, X, R, CH = dims
    NCH = R // CH
    QT = R // 256
    NU, ND = Z // 2, Z // 2 - 1
    ep = lax.axis_index("ep")
    tp = lax.axis_index("tp")
    z, core = ep // 2, ep % 2
    y, x = tp // X, tp % X
    up = (lax.rem(ep + 2, 2 * Z), tp)
    down = (lax.rem(ep + 2 * Z - 2, 2 * Z), tp)
    partner = (2 * z + 1 - core, tp)

    def x_peer(k):
        return (ep, y * X + lax.rem(x + k, X))

    def y_peer(k):
        return (ep, lax.rem(y + k, Y) * X + x)

    barrier = pltpu.get_barrier_semaphore()
    peers = [x_peer(k) for k in range(1, X)] + [y_peer(k) for k in range(1, Y)]
    for peer in peers:
        pl.semaphore_signal(barrier, inc=1, device_id=peer, device_id_type=MESH)

    def greet(k, carry):
        pl.semaphore_signal(barrier, inc=1, device_id=(lax.rem(ep + k, 2 * Z), tp), device_id_type=MESH)
        return carry

    lax.fori_loop(1, 2 * Z, greet, 0)
    pl.semaphore_wait(barrier, len(peers) + 2 * Z - 1)

    def copy(src, dst, ssem, rsem, dev):
        return pltpu.make_async_remote_copy(
            src_ref=src, dst_ref=dst, send_sem=ssem, recv_sem=rsem,
            device_id=dev, device_id_type=MESH)

    def first(c, slot, dev):
        return copy(kv_ref.at[:, pl.ds(c * CH, CH)], kv.at[slot, c, 0],
                    ring_send.at[slot, c], ring_recv.at[slot, c], dev)

    def first_pair(c):
        return copy(kv_ref.at[:, pl.ds(c * CH, CH)], kv.at[0, c, 1],
                    pair_send.at[0, c], pair_recv.at[0, c], partner)

    def onward(slot, c, dev):
        return copy(kv.at[slot, c, 0], kv.at[slot + 1, c, 0],
                    ring_send.at[slot + 1, c], ring_recv.at[slot + 1, c], dev)

    def to_pair(slot, c):
        return copy(kv.at[slot, c, 0], kv.at[slot, c, 1],
                    pair_send.at[slot, c], pair_recv.at[slot, c], partner)

    (send_weights, dispatch, shared_first, shared_second, gather_rows, first_products,
     second_products, combine, finish, drain_experts) = expert_stages(
        (2 * Z, Y, X, expert_ins[0].shape[0]), copy, x_peer, y_peer, expert_ins, moe_ref, expert_scratch_refs)

    for c in range(NCH):
        @pl.when(z < Z - 1)
        def _():
            first(c, 1, up).start()

        @pl.when(z < ND)
        def _():
            first(c, NU + 1, down).start()

        first_pair(c).start()

    send_weights()
    dispatch()
    q_all = jnp.transpose(qT_ref[...].astype(jnp.float32)) * (HEAD ** -0.5 * LOG2E)
    q_hi, q_mid, q_lo = in_three(q_all)
    q_one = jnp.where(lax.broadcasted_iota(jnp.int32, (R, HEAD), 1) < 3, 1.0, 0.0).astype(jnp.bfloat16)
    qs[:, 0:128] = jnp.concatenate([q_hi, q_mid], axis=1)
    qs[:, 128:256] = jnp.concatenate([q_lo, q_one], axis=1)
    mx[...] = jnp.full(mx.shape, neg_fill, jnp.float32)
    acc[...] = jnp.zeros(acc.shape, jnp.float32)
    wb[...] = jnp.zeros(wb.shape, jnp.bfloat16)

    def place(h, _):
        part = w_ref[pl.ds(pl.multiple_of(h * HEAD, HEAD), HEAD), :]
        wb[pl.ds(pl.multiple_of(h * 128, 128), HEAD), 0:128] = part
        wb[pl.ds(pl.multiple_of(h * 128 + HEAD, HEAD), HEAD), 128:256] = part
        return 0

    lax.fori_loop(0, w_ref.shape[0] // HEAD, place, 0)

    shared_first()
    first_row = pl.multiple_of(ep * R, 128)
    base_gate = cg_ref[:, pl.ds(first_row, 128)][:, 0:1]

    def gate_of(block, c):
        at = pl.multiple_of(block * R + c * CH, 128)
        return (base_gate - cg_ref[:, pl.ds(at, CH)]) * LOG2E

    def score_side(pair, gate):
        hi, mid, lo = in_three(gate)
        row = lax.broadcasted_iota(jnp.int32, (HEAD, CH), 0)
        hi, mid, lo = (piece.astype(jnp.float32) for piece in (hi, mid, lo))
        gates = jnp.where(row == 0, hi, jnp.where(row == 1, mid, jnp.where(row == 2, lo, 0.0)))
        keys = pair[0:HEAD, :]
        return jnp.concatenate([keys, keys, keys, gates.astype(jnp.bfloat16)], axis=0)

    def value_side(pair):
        return jnp.concatenate([jnp.ones((HEAD, CH), jnp.bfloat16), pair[HEAD:2 * HEAD, :]], axis=0)

    def update(i, sides, masked=False):
        rows = slice(i * 256, (i + 1) * 256)
        q = qs[rows, :]
        logits = [jnp.dot(q, keys, preferred_element_type=jnp.float32) for keys, _ in sides]
        if masked:
            qi = lax.broadcasted_iota(jnp.int32, logits[0].shape, 0)
            ki = lax.broadcasted_iota(jnp.int32, logits[0].shape, 1)
            logits[0] = jnp.where(ki <= qi, logits[0], neg_fill)
        tops = [s[:, at:at + 128] for s in logits for at in range(0, CH, 128)]
        top = tops[0]
        for s in tops[1:]:
            top = jnp.maximum(top, s)
        old = mx[rows, :]
        new = jnp.maximum(old, jnp.max(top, axis=1, keepdims=True))
        wide = jnp.concatenate([new] * (CH // 128), axis=1)
        total = acc[rows, :] * jnp.exp2(old - new)
        for s, (_, values) in zip(logits, sides):
            p = jnp.exp2(s - wide).astype(jnp.bfloat16)
            total = total + lax.dot_general(
                p, values, (((1,), (1,)), ((), ())), preferred_element_type=jnp.float32)
        acc[rows, :] = total
        mx[rows, :] = new

    def sides_of(pair, block, c):
        return score_side(pair, gate_of(block, c)), value_side(pair)

    for c in range(NCH):
        side = sides_of(kv_ref[:, c * CH:(c + 1) * CH], ep, c)
        for i in range(c, QT):
            update(i, [side], i == c)

    for c in range(NCH):
        to = first_pair(c)
        to.wait_recv()

    @pl.when(core == 1)
    def _():
        for c in range(NCH):
            side = sides_of(kv[0, c, 1], ep - 1, c)
            for i in range(QT):
                update(i, [side])

    def issue(s, c):
        @pl.when(s <= z)
        def _():
            onward(s - 1, c, up).wait_recv()
            to_pair(s, c).start()

            @pl.when(jnp.logical_and(s < NU, z < Z - 1))
            def _():
                onward(s, c, up).start()

        @pl.when(jnp.logical_and(s <= ND, lax.rem(z + s, Z) < ND))
        def _():
            onward(NU + s - 1, c, down).wait_recv()

            @pl.when(s < ND)
            def _():
                onward(NU + s, c, down).start()

            @pl.when(z + s >= Z)
            def _():
                to_pair(NU + s, c).start()

    def attend(slot, c, chip):
        sides = [sides_of(kv[slot, c, 0], 2 * chip + core, c), sides_of(kv[slot, c, 1], 2 * chip + 1 - core, c)]
        for i in range(QT):
            update(i, sides)

    def consume(s, c):
        @pl.when(s <= z)
        def _():
            to_pair(s, c).wait_recv()
            attend(s, c, z - s)

        @pl.when(jnp.logical_and(s <= ND, z + s >= Z))
        def _():
            to_pair(NU + s, c).wait_recv()
            attend(NU + s, c, z + s - Z)

    steps = NU * NCH

    def step(t, _):
        @pl.when(t < steps)
        def _():
            issue(t // NCH + 1, t % NCH)

        for at, stage in zip(stops, (shared_second, gather_rows, first_products, second_products)):
            @pl.when(t == at)
            def _():
                stage()

        @pl.when(t >= 1)
        def _():
            consume((t - 1) // NCH + 1, (t - 1) % NCH)

        return 0

    lax.fori_loop(0, steps + 1, step, 0)

    quarter, half = R // 4, R // 2
    low = lax.broadcasted_iota(jnp.int32, (quarter, 128), 1) < HEAD

    def finished(at):
        a = acc[at:at + quarter, :]
        return a / pltpu.roll(a, HEAD, 1)

    for h in range(2):
        first_half = pltpu.roll(finished(h * quarter), HEAD, 1)
        second_half = finished(half + h * quarter)
        hg[h, y, x] = jnp.where(low, first_half, second_half).astype(jnp.bfloat16)

    def spread(h, phase, k):
        along_x = (h == 0) == (phase == 0)
        dev = x_peer(k) if along_x else y_peer(k)
        if phase == 0:
            ref = hg.at[h, y, x]
        elif along_x:
            ref = hg.at[h, :, x]
        else:
            ref = hg.at[h, y]
        return copy(ref, ref, head_send.at[h, phase, k], head_recv.at[h, phase, k], dev)

    def spread_in(h, phase, k):
        along_x = (h == 0) == (phase == 0)
        n = X if along_x else Y
        src_x = lax.rem(x + X - k, X)
        src_y = lax.rem(y + Y - k, Y)
        if phase == 0:
            ref = hg.at[h, y, src_x] if along_x else hg.at[h, src_y, x]
        elif along_x:
            ref = hg.at[h, :, src_x]
        else:
            ref = hg.at[h, src_y]
        return copy(ref, ref, head_send.at[h, phase, k], head_recv.at[h, phase, k], partner)

    def count(h, phase):
        return X if (h == 0) == (phase == 0) else Y

    for phase in range(2):
        for h in range(2):
            if phase == 1:
                for k in range(1, count(h, 0)):
                    spread_in(h, 0, k).wait_recv()
            for k in range(1, count(h, phase)):
                spread(h, phase, k).start()
        if phase == 0:
            combine()
        else:
            finish()

    for h in range(2):
        for k in range(1, count(h, 1)):
            spread_in(h, 1, k).wait_recv()
        heads = X * Y
        flat = hg.at[h]
        total = jnp.zeros((quarter, 256), jnp.float32)
        for pair in range(heads // 2):
            a, b = 2 * pair, 2 * pair + 1
            lhs = jnp.concatenate([flat[a // X, a % X], flat[b // X, b % X]], axis=1)
            total = total + jnp.dot(lhs, wb[pair * 256:(pair + 1) * 256, :],
                                    preferred_element_type=jnp.float32)
        out_ref[h * quarter:(h + 1) * quarter, :] = total[:, 0:128].astype(jnp.bfloat16)
        out_ref[half + h * quarter:half + (h + 1) * quarter, :] = total[:, 128:256].astype(jnp.bfloat16)

    for c in range(NCH):
        @pl.when(z < Z - 1)
        def _():
            first(c, 1, up).wait_send()

        @pl.when(z < ND)
        def _():
            first(c, NU + 1, down).wait_send()

        first_pair(c).wait_send()

    def drain(s, _):
        for c in range(NCH):
            @pl.when(s <= z)
            def _():
                to_pair(s, c).wait_send()

                @pl.when(jnp.logical_and(s < NU, z < Z - 1))
                def _():
                    onward(s, c, up).wait_send()

            @pl.when(jnp.logical_and(s <= ND, lax.rem(z + s, Z) < ND))
            def _():
                @pl.when(s < ND)
                def _():
                    onward(NU + s, c, down).wait_send()

                @pl.when(z + s >= Z)
                def _():
                    to_pair(NU + s, c).wait_send()
        return 0

    lax.fori_loop(1, NU + 1, drain, 0)
    drain_experts()
    for phase in range(2):
        for h in range(2):
            for k in range(1, count(h, phase)):
                spread(h, phase, k).wait_send()


def dot_nn(a, b):
    return jnp.dot(a, b, preferred_element_type=jnp.float32)


def dot_nt(a, b):
    return lax.dot_general(a, b, (((1,), (1,)), ((), ())), preferred_element_type=jnp.float32)


def dot_tn(a, b):
    return lax.dot_general(a, b, (((0,), (0,)), ((), ())), preferred_element_type=jnp.float32)


def iota(shape, dim):
    return lax.broadcasted_iota(jnp.int32, shape, dim)


def as_bf16(flags):
    return jnp.where(flags, 1.0, 0.0).astype(jnp.bfloat16)


def expert_stages(dims, copy, x_peer, y_peer, ins, out_ref, scratch):
    n_ep, Y, X, T = dims
    x_in, gain_in, routes_in, routes_t_in, share_in, gate_in, up_in, down_in, sgate_in, sup_in, sdown_in = ins
    (normed, ob, rb, fa, gw, uw, dw, ha, ro, cb, ps, pr, sh,
     z_sems, w_sems, y_sems, p_sems, s_sems) = scratch
    ep = lax.axis_index("ep")
    tp = lax.axis_index("tp")
    y, x = tp // X, tp % X
    D = normed.shape[1]
    DY = D // Y
    B8 = 8 * n_ep
    HU = gate_in.shape[1]

    def ep_peer(k):
        return (lax.rem(ep + k, n_ep), tp)

    def ep_from(k):
        return lax.rem(ep + n_ep - k, n_ep)

    def x_to(k):
        return lax.rem(x + k, X)

    def x_from(k):
        return lax.rem(x + X - k, X)

    def y_from(k):
        return lax.rem(y + Y - k, Y)

    def weight_copies(k, incoming):
        to, place = x_to(k), (x_from(k) if incoming else x)
        rows = pl.ds(pl.multiple_of(place * HU, HU), HU)
        return [
            copy(gate_in.at[to], gw.at[rows], w_sems.at[0, 0, k], w_sems.at[1, 0, k], x_peer(k)),
            copy(up_in.at[to], uw.at[rows], w_sems.at[0, 1, k], w_sems.at[1, 1, k], x_peer(k)),
            copy(down_in.at[to], dw.at[place], w_sems.at[0, 2, k], w_sems.at[1, 2, k], x_peer(k)),
        ]

    def send_weights():
        for k in range(1, X):
            for c in weight_copies(k, False):
                c.start()
        rows = pl.ds(pl.multiple_of(x * HU, HU), HU)
        gw[rows, :] = gate_in[x]
        uw[rows, :] = up_in[x]
        dw[x] = down_in[x]

    def out_copy(k):
        to = lax.rem(ep + k, n_ep)
        return copy(ob.at[to], rb.at[ep], z_sems.at[0, 0, k], z_sems.at[0, 1, k], ep_peer(k))

    def in_copy(k):
        return copy(ob.at[ep], rb.at[ep_from(k)], z_sems.at[0, 0, k], z_sems.at[0, 1, k], ep_peer(k))

    def back_copy(k):
        to = lax.rem(ep + k, n_ep)
        return copy(ro.at[to], cb.at[ep], z_sems.at[1, 0, k], z_sems.at[1, 1, k], ep_peer(k))

    def returned_copy(k):
        return copy(ro.at[ep], cb.at[ep_from(k)], z_sems.at[1, 0, k], z_sems.at[1, 1, k], ep_peer(k))

    def each(first, last, fn):
        def body(k, carry):
            fn(k)
            return carry
        lax.fori_loop(first, last, body, 0)

    def row_copy(k):
        return copy(fa.at[y], fa.at[y], y_sems.at[0, 0, k], y_sems.at[0, 1, k], y_peer(k))

    def row_in(k):
        return copy(fa.at[y], fa.at[y_from(k)], y_sems.at[0, 0, k], y_sems.at[0, 1, k], y_peer(k))

    def hid_copy(k):
        return copy(ha.at[y], ha.at[y], y_sems.at[1, 0, k], y_sems.at[1, 1, k], y_peer(k))

    def hid_in(k):
        return copy(ha.at[y], ha.at[y_from(k)], y_sems.at[1, 0, k], y_sems.at[1, 1, k], y_peer(k))

    def part_copy(k):
        return copy(ps.at[x_to(k)], pr.at[x], p_sems.at[0, k], p_sems.at[1, k], x_peer(k))

    def part_in(k):
        return copy(ps.at[x], pr.at[x_from(k)], p_sems.at[0, k], p_sems.at[1, k], x_peer(k))

    def share_x(k):
        return copy(sh.at[y, x], sh.at[y, x], s_sems.at[0, 0, k], s_sems.at[0, 1, k], x_peer(k))

    def share_x_in(k):
        return copy(sh.at[y, x], sh.at[y, x_from(k)], s_sems.at[0, 0, k], s_sems.at[0, 1, k], x_peer(k))

    def share_y(k):
        return copy(sh.at[y], sh.at[y], s_sems.at[1, 0, k], s_sems.at[1, 1, k], y_peer(k))

    def share_y_in(k):
        return copy(sh.at[y], sh.at[y_from(k)], s_sems.at[1, 0, k], s_sems.at[1, 1, k], y_peer(k))

    def pick(wide):
        row = iota((B8, 128), 0) % 8
        total = jnp.zeros((B8, 128), jnp.float32)
        for c in range(X):
            total = total + jnp.where(row == c, wide[:, c * 128:(c + 1) * 128], 0.0)
        return total

    def to_tiles(value):
        return value.reshape(n_ep, 8, 128).astype(jnp.bfloat16)

    def from_tiles(tiles):
        return tiles.astype(jnp.float32).reshape(B8, 128).astype(jnp.bfloat16)

    def ninth(tile, c):
        chosen = as_bf16(iota((n_ep, B8), 1) == 8 * iota((n_ep, B8), 0) + c)
        return dot_nn(chosen, tile)

    def spread_rows(value):
        expand = as_bf16(iota((B8, n_ep), 0) // 8 == iota((B8, n_ep), 1))
        return dot_nn(expand, value)

    def dispatch():
        rows = x_in[...].astype(jnp.float32)
        mean = jnp.mean(rows * rows, axis=1, keepdims=True)
        normed[...] = (rows * lax.rsqrt(mean + norm_eps) * gain_in[...]).astype(jnp.bfloat16)
        named = iota((n_ep, T), 0) * X + x
        hit = named == routes_t_in[0:1, :]
        for j in range(1, TOP):
            hit = jnp.logical_or(hit, named == routes_t_in[j:j + 1, :])
        before = as_bf16(iota((T, T), 0) < iota((T, T), 1))
        rank = dot_nn(as_bf16(hit), before)
        place = spread_rows(jnp.where(hit, rank, -1.0).astype(jnp.bfloat16))
        mine = normed[:, pl.ds(pl.multiple_of(y * DY, 128), DY)]
        slot = (iota((B8, T), 0) % 8).astype(jnp.float32)
        main = dot_nn(as_bf16(place == slot), mine)
        last = pick(dot_nn(as_bf16(place == 8.0), mine))
        for c in range(X):
            ob[:, c] = to_tiles(main[:, c * 128:(c + 1) * 128])
        ob[:, X] = to_tiles(last)
        each(1, n_ep, lambda k: out_copy(k).start())
        rb[ep] = ob[ep]

    def shared_first():
        gate = dot_nt(sgate_in[...], normed[...])
        up = dot_nt(sup_in[...], normed[...])
        sh[y, x] = (gate / (1.0 + jnp.exp(-gate)) * up).astype(jnp.bfloat16)
        for k in range(1, X):
            share_x(k).start()

    def shared_second():
        for k in range(1, X):
            share_x_in(k).wait_recv()
        for k in range(1, Y):
            share_y(k).start()

    def gather_rows():
        each(1, n_ep, lambda k: in_copy(k).wait_recv())
        tile = from_tiles(rb[:, X])
        for c in range(X):
            fa[y, 0:B8, c * 128:(c + 1) * 128] = from_tiles(rb[:, c])
            fa[y, B8:B8 + n_ep, c * 128:(c + 1) * 128] = ninth(tile, c).astype(jnp.bfloat16)
        for k in range(1, Y):
            row_copy(k).start()

    def first_products():
        for k in range(1, X):
            for c in weight_copies(k, True):
                c.wait_recv()
        for k in range(1, Y):
            row_in(k).wait_recv()
        gate = jnp.zeros((B8 + n_ep, X * HU), jnp.float32)
        up = jnp.zeros((B8 + n_ep, X * HU), jnp.float32)
        for part in range(Y):
            piece = fa[part]
            gate = gate + dot_nt(piece, gw[:, part * DY:(part + 1) * DY])
            up = up + dot_nt(piece, uw[:, part * DY:(part + 1) * DY])
        ha[y] = (gate / (1.0 + jnp.exp(-gate)) * up).astype(jnp.bfloat16)
        for k in range(1, Y):
            hid_copy(k).start()

    def second_products():
        for k in range(1, Y):
            hid_in(k).wait_recv()
        hidden = jnp.concatenate([ha[part] for part in range(Y)], axis=1)
        ends = []
        for c in range(X):
            result = dot_nn(hidden, dw[c])
            ro[:, c] = to_tiles(result[0:B8])
            ends.append(result[B8:B8 + n_ep].astype(jnp.bfloat16))
        ro[:, X] = to_tiles(pick(spread_rows(jnp.concatenate(ends, axis=1))))
        each(1, n_ep, lambda k: back_copy(k).start())
        cb[ep] = ro[ep]

    def combine():
        named = iota((T, n_ep), 1) * X + x
        hit = jnp.zeros((T, n_ep), jnp.float32)
        weight = jnp.zeros((T, n_ep), jnp.float32)
        for j in range(TOP):
            same = named == routes_in[:, j:j + 1]
            hit = hit + jnp.where(same, 1.0, 0.0)
            weight = weight + jnp.where(same, share_in[:, j:j + 1], 0.0)
        before = as_bf16(iota((T, T), 1) < iota((T, T), 0))
        rank = dot_nn(before, hit.astype(jnp.bfloat16))
        rank = jnp.where(hit > 0.0, rank, -1.0)
        high = weight.astype(jnp.bfloat16)
        low = (weight - high.astype(jnp.float32)).astype(jnp.bfloat16)
        widen = as_bf16(iota((n_ep, B8), 1) // 8 == iota((n_ep, B8), 0))
        at = dot_nn(rank.astype(jnp.bfloat16), widen) == (iota((T, B8), 1) % 8).astype(jnp.float32)
        end = rank == 8.0
        each(1, n_ep, lambda k: returned_copy(k).wait_recv())
        main = jnp.concatenate([from_tiles(cb[:, c]) for c in range(X)], axis=1)
        tile = from_tiles(cb[:, X])
        last = jnp.concatenate([ninth(tile, c).astype(jnp.bfloat16) for c in range(X)], axis=1)
        total = jnp.zeros((T, DY), jnp.float32)
        for piece in (high, low):
            scaled = jnp.where(at, dot_nn(piece, widen), 0.0).astype(jnp.bfloat16)
            total = total + dot_nn(scaled, main)
            total = total + dot_nn(jnp.where(end, piece.astype(jnp.float32), 0.0).astype(jnp.bfloat16), last)
        for c in range(X):
            ps[c] = total[:, c * 128:(c + 1) * 128]
        for k in range(1, X):
            part_copy(k).start()

    def finish():
        for k in range(1, Y):
            share_y_in(k).wait_recv()
        hidden = jnp.concatenate([sh[a, b] for a in range(Y) for b in range(X)], axis=0)
        total = dot_tn(hidden, sdown_in[...])
        for k in range(1, X):
            part_in(k).wait_recv()
        total = total + ps[x]
        for k in range(1, X):
            total = total + pr[x_from(k)]
        out_ref[...] = total.astype(jnp.bfloat16)

    def drain():
        each(1, n_ep, lambda k: out_copy(k).wait_send())
        each(1, n_ep, lambda k: back_copy(k).wait_send())
        for k in range(1, X):
            for c in weight_copies(k, False):
                c.wait_send()
            share_x(k).wait_send()
            part_copy(k).wait_send()
        for k in range(1, Y):
            share_y(k).wait_send()
            row_copy(k).wait_send()
            hid_copy(k).wait_send()

    return (send_weights, dispatch, shared_first, shared_second, gather_rows, first_products,
            second_products, combine, finish, drain)


def expert_scratch(n_ep, Y, X, T, D, HU, FF):
    B8 = 8 * n_ep
    tiles = (n_ep, X + 1, 8, 128)
    bf16 = jnp.bfloat16
    return [
        pltpu.VMEM((T, D), bf16),
        pltpu.VMEM(tiles, bf16),
        pltpu.VMEM(tiles, bf16),
        pltpu.VMEM((Y, B8 + n_ep, D // Y), bf16),
        pltpu.VMEM((X * HU, D), bf16),
        pltpu.VMEM((X * HU, D), bf16),
        pltpu.VMEM((X, FF, 128), bf16),
        pltpu.VMEM((Y, B8 + n_ep, X * HU), bf16),
        pltpu.VMEM(tiles, bf16),
        pltpu.VMEM(tiles, bf16),
        pltpu.VMEM((X, T, 128), jnp.float32),
        pltpu.VMEM((X, T, 128), jnp.float32),
        pltpu.VMEM((Y, X, HU, T), bf16),
        pltpu.SemaphoreType.DMA((2, 2, n_ep)),
        pltpu.SemaphoreType.DMA((2, 3, X)),
        pltpu.SemaphoreType.DMA((2, 2, Y)),
        pltpu.SemaphoreType.DMA((2, X)),
        pltpu.SemaphoreType.DMA((2, 2, 4)),
    ]


def local(
    query_rows,
    key_rows,
    value_rows,
    cum_gate,
    out_weight,
    moe_input,
    moe_gain,
    routes,
    route_weight,
    expert_gate,
    expert_up,
    expert_down,
    shared_gate,
    shared_up,
    shared_down,
):
    n_ep, n_tp = lax.axis_size("ep"), lax.axis_size("tp")
    X = expert_gate.shape[0]
    Y = n_tp // X
    Z = n_ep // 2
    R = query_rows.shape[0]
    CH = 256
    T, D = moe_input.shape
    HU = expert_gate.shape[2]
    kv = jnp.concatenate([key_rows.T, value_rows.T], axis=0)
    vm = pl.BlockSpec(memory_space=pltpu.VMEM)
    step = pl.pallas_call(
        functools.partial(step_kernel, (Z, Y, X, R, CH), STOPS),
        out_shape=(
            jax.ShapeDtypeStruct((R, out_weight.shape[1]), jnp.bfloat16),
            jax.ShapeDtypeStruct((T, out_weight.shape[1]), jnp.bfloat16),
        ),
        in_specs=[vm] * 15,
        out_specs=(vm, vm),
        scratch_shapes=[
            pltpu.VMEM((Z, R // CH, 2, 2 * HEAD, CH), jnp.bfloat16),
            pltpu.VMEM((R, 256), jnp.bfloat16),
            pltpu.VMEM((R, 128), jnp.float32),
            pltpu.VMEM((R, 128), jnp.float32),
            pltpu.VMEM((2, Y, X, R // 4, 128), jnp.bfloat16),
            pltpu.VMEM((n_tp * 128, 256), jnp.bfloat16),
            pltpu.SemaphoreType.DMA((Z, R // CH)),
            pltpu.SemaphoreType.DMA((Z, R // CH)),
            pltpu.SemaphoreType.DMA((Z, R // CH)),
            pltpu.SemaphoreType.DMA((Z, R // CH)),
            pltpu.SemaphoreType.DMA((2, 2, 4)),
            pltpu.SemaphoreType.DMA((2, 2, 4)),
        ]
        + expert_scratch(n_ep, Y, X, T, D, HU, expert_down.shape[1]),
        compiler_params=pltpu.CompilerParams(
            collective_id=0, has_side_effects=True, vmem_limit_bytes=56 * 1024 * 1024
        ),
    )
    return step(
        query_rows.T,
        kv,
        cum_gate,
        out_weight,
        moe_input,
        moe_gain[None, :],
        routes,
        routes.T,
        route_weight,
        expert_gate.swapaxes(1, 2),
        expert_up.swapaxes(1, 2),
        expert_down,
        shared_gate.T,
        shared_up.T,
        shared_down,
    )


def solution(mesh):
    placed = (
        P("ep", "tp"),
        P("ep", "tp"),
        P("ep", "tp"),
        P("tp", None),
        P(None, "tp"),
        P("ep", None),
        P(),
        P("ep", None),
        P("ep", None),
        P("ep", None, "tp"),
        P("ep", None, "tp"),
        P("ep", None, "tp"),
        P(None, "tp"),
        P(None, "tp"),
        P(None, "tp"),
    )
    return jax.shard_map(
        local, mesh=mesh, in_specs=placed, out_specs=(P("ep", "tp"), P("ep", "tp")), check_vma=False
    )
```

```python
import functools
import jax
import jax.numpy as jnp
from jax import lax
from jax.experimental import pallas as pl
from jax.experimental.pallas import tpu as pltpu
from jax.sharding import PartitionSpec as P

HEAD = 64
TOP = 3
LOG2E = 1.4426950408889634
MESH = pl.DeviceIdType.MESH
STOPS = (2, 7, 12, 15)
neg_fill = -1e30
norm_eps = 1e-06


def in_three(value):
    hi = value.astype(jnp.bfloat16)
    left = value - hi.astype(jnp.float32)
    mid = left.astype(jnp.bfloat16)
    low = (left - mid.astype(jnp.float32)).astype(jnp.bfloat16)
    return hi, mid, low


def step_kernel(dims, stops, *refs):
    qT_ref, kT_ref, vT_ref, cg_ref, w_ref = refs[0:5]
    expert_ins = refs[5:15]
    out_ref, moe_ref = refs[15:17]
    kv, qs, acc, mx, hg, wb, ring_send, ring_recv, pair_send, pair_recv, head_send, head_recv = refs[17:29]
    expert_scratch_refs = refs[29:]
    Z, Y, X, R, CH = dims
    NCH = R // CH
    QT = R // 256
    NU, ND = Z // 2, Z // 2 - 1
    ep = lax.axis_index("ep")
    tp = lax.axis_index("tp")
    z, core = ep // 2, ep % 2
    y, x = tp // X, tp % X
    up = (lax.rem(ep + 2, 2 * Z), tp)
    down = (lax.rem(ep + 2 * Z - 2, 2 * Z), tp)
    partner = (2 * z + 1 - core, tp)

    def x_peer(k):
        return (ep, y * X + lax.rem(x + k, X))

    def y_peer(k):
        return (ep, lax.rem(y + k, Y) * X + x)

    barrier = pltpu.get_barrier_semaphore()
    peers = [x_peer(k) for k in range(1, X)] + [y_peer(k) for k in range(1, Y)]
    for peer in peers:
        pl.semaphore_signal(barrier, inc=1, device_id=peer, device_id_type=MESH)

    def greet(k, carry):
        pl.semaphore_signal(barrier, inc=1, device_id=(lax.rem(ep + k, 2 * Z), tp), device_id_type=MESH)
        return carry

    lax.fori_loop(1, 2 * Z, greet, 0)

    def copy(src, dst, ssem, rsem, dev):
        return pltpu.make_async_remote_copy(
            src_ref=src, dst_ref=dst, send_sem=ssem, recv_sem=rsem,
            device_id=dev, device_id_type=MESH)

    def halves(c, target, ssem, rsem, dev):
        keys = copy(kT_ref.at[:, pl.ds(c * CH, CH)], target.at[0:HEAD], ssem, rsem, dev)
        values = copy(vT_ref.at[:, pl.ds(c * CH, CH)], target.at[HEAD:2 * HEAD], ssem, rsem, dev)
        keys.start()
        values.start()

    def start_first(c, slot, dev):
        halves(c, kv.at[slot, c, 0], ring_send.at[slot, c], ring_recv.at[slot, c], dev)

    def start_first_pair(c):
        halves(c, kv.at[0, c, 1], pair_send.at[0, c], pair_recv.at[0, c], partner)

    def first(c, slot, dev):
        return copy(kv.at[slot, c, 0], kv.at[slot, c, 0], ring_send.at[slot, c], ring_recv.at[slot, c], dev)

    def first_pair(c):
        return copy(kv.at[0, c, 1], kv.at[0, c, 1], pair_send.at[0, c], pair_recv.at[0, c], partner)

    def onward(slot, c, dev):
        return copy(kv.at[slot, c, 0], kv.at[slot + 1, c, 0],
                    ring_send.at[slot + 1, c], ring_recv.at[slot + 1, c], dev)

    def to_pair(slot, c):
        return copy(kv.at[slot, c, 0], kv.at[slot, c, 1],
                    pair_send.at[slot, c], pair_recv.at[slot, c], partner)

    (keep_weights, send_weights, dispatch, send_rows, shared_first, send_shared, shared_second,
     gather_rows, first_products, second_products, combine, finish, drain_experts) = expert_stages(
        (2 * Z, Y, X, expert_ins[0].shape[0]), copy, x_peer, y_peer, expert_ins, moe_ref, expert_scratch_refs)

    dispatch()
    shared_first()
    keep_weights()
    q_all = jnp.transpose(qT_ref[...].astype(jnp.float32)) * (HEAD ** -0.5 * LOG2E)
    q_hi, q_mid, q_lo = in_three(q_all)
    q_one = jnp.where(lax.broadcasted_iota(jnp.int32, (R, HEAD), 1) < 3, 1.0, 0.0).astype(jnp.bfloat16)
    qs[:, 0:128] = jnp.concatenate([q_hi, q_mid], axis=1)
    qs[:, 128:256] = jnp.concatenate([q_lo, q_one], axis=1)
    mx[...] = jnp.full(mx.shape, neg_fill, jnp.float32)
    acc[...] = jnp.zeros(acc.shape, jnp.float32)
    wb[...] = jnp.zeros(wb.shape, jnp.bfloat16)

    def place(h, _):
        part = w_ref[pl.ds(pl.multiple_of(h * HEAD, HEAD), HEAD), :]
        wb[pl.ds(pl.multiple_of(h * 128, 128), HEAD), 0:128] = part
        wb[pl.ds(pl.multiple_of(h * 128 + HEAD, HEAD), HEAD), 128:256] = part
        return 0

    lax.fori_loop(0, w_ref.shape[0] // HEAD, place, 0)

    first_row = pl.multiple_of(ep * R, 128)
    base_gate = cg_ref[:, pl.ds(first_row, 128)][:, 0:1]

    def gate_of(block, c):
        at = pl.multiple_of(block * R + c * CH, 128)
        return (base_gate - cg_ref[:, pl.ds(at, CH)]) * LOG2E

    def score_side(pair, gate):
        hi, mid, lo = in_three(gate)
        row = lax.broadcasted_iota(jnp.int32, (HEAD, CH), 0)
        hi, mid, lo = (piece.astype(jnp.float32) for piece in (hi, mid, lo))
        gates = jnp.where(row == 0, hi, jnp.where(row == 1, mid, jnp.where(row == 2, lo, 0.0)))
        keys = pair[0:HEAD, :]
        return jnp.concatenate([keys, keys, keys, gates.astype(jnp.bfloat16)], axis=0)

    def value_side(pair):
        return jnp.concatenate([jnp.ones((HEAD, CH), jnp.bfloat16), pair[HEAD:2 * HEAD, :]], axis=0)

    def update(i, sides, masked=False):
        rows = slice(i * 256, (i + 1) * 256)
        q = qs[rows, :]
        logits = [jnp.dot(q, keys, preferred_element_type=jnp.float32) for keys, _ in sides]
        if masked:
            qi = lax.broadcasted_iota(jnp.int32, logits[0].shape, 0)
            ki = lax.broadcasted_iota(jnp.int32, logits[0].shape, 1)
            logits[0] = jnp.where(ki <= qi, logits[0], neg_fill)
        tops = [s[:, at:at + 128] for s in logits for at in range(0, CH, 128)]
        top = tops[0]
        for s in tops[1:]:
            top = jnp.maximum(top, s)
        old = mx[rows, :]
        new = jnp.maximum(old, jnp.max(top, axis=1, keepdims=True))
        wide = jnp.concatenate([new] * (CH // 128), axis=1)
        total = acc[rows, :] * jnp.exp2(old - new)
        for s, (_, values) in zip(logits, sides):
            p = jnp.exp2(s - wide).astype(jnp.bfloat16)
            total = total + lax.dot_general(
                p, values, (((1,), (1,)), ((), ())), preferred_element_type=jnp.float32)
        acc[rows, :] = total
        mx[rows, :] = new

    def sides_of(pair, block, c):
        return score_side(pair, gate_of(block, c)), value_side(pair)

    for c in range(NCH):
        side = sides_of(jnp.concatenate([kT_ref[:, c * CH:(c + 1) * CH], vT_ref[:, c * CH:(c + 1) * CH]], axis=0), ep, c)
        for i in range(c, QT):
            update(i, [side], i == c)

    pl.semaphore_wait(barrier, len(peers) + 2 * Z - 1)
    for c in range(NCH):
        @pl.when(z < Z - 1)
        def _():
            start_first(c, 1, up)

        @pl.when(z < ND)
        def _():
            start_first(c, NU + 1, down)

        start_first_pair(c)

    send_rows()
    send_weights()
    send_shared()
    for c in range(NCH):
        first_pair(c).wait_recv()

    @pl.when(core == 1)
    def _():
        for c in range(NCH):
            side = sides_of(kv[0, c, 1], ep - 1, c)
            for i in range(QT):
                update(i, [side])

    def issue(s, c):
        @pl.when(s <= z)
        def _():
            onward(s - 1, c, up).wait_recv()
            to_pair(s, c).start()

            @pl.when(jnp.logical_and(s < NU, z < Z - 1))
            def _():
                onward(s, c, up).start()

        @pl.when(jnp.logical_and(s <= ND, lax.rem(z + s, Z) < ND))
        def _():
            onward(NU + s - 1, c, down).wait_recv()

            @pl.when(s < ND)
            def _():
                onward(NU + s, c, down).start()

            @pl.when(z + s >= Z)
            def _():
                to_pair(NU + s, c).start()

    def attend(slot, c, chip):
        sides = [sides_of(kv[slot, c, 0], 2 * chip + core, c), sides_of(kv[slot, c, 1], 2 * chip + 1 - core, c)]
        for i in range(QT):
            update(i, sides)

    def consume(s, c):
        @pl.when(s <= z)
        def _():
            to_pair(s, c).wait_recv()
            attend(s, c, z - s)

        @pl.when(jnp.logical_and(s <= ND, z + s >= Z))
        def _():
            to_pair(NU + s, c).wait_recv()
            attend(NU + s, c, z + s - Z)

    steps = NU * NCH

    def step(t, _):
        @pl.when(t < steps)
        def _():
            issue(t // NCH + 1, t % NCH)

        for at, stage in zip(stops, (shared_second, gather_rows, first_products, second_products)):
            @pl.when(t == at)
            def _():
                stage()

        @pl.when(t >= 1)
        def _():
            consume((t - 1) // NCH + 1, (t - 1) % NCH)

        return 0

    lax.fori_loop(0, steps + 1, step, 0)

    quarter, half = R // 4, R // 2
    low = lax.broadcasted_iota(jnp.int32, (quarter, 128), 1) < HEAD

    def finished(at):
        a = acc[at:at + quarter, :]
        return a / pltpu.roll(a, HEAD, 1)

    for h in range(2):
        first_half = pltpu.roll(finished(h * quarter), HEAD, 1)
        second_half = finished(half + h * quarter)
        hg[h, y, x] = jnp.where(low, first_half, second_half).astype(jnp.bfloat16)

    def spread(h, phase, k):
        along_x = (h == 0) == (phase == 0)
        dev = x_peer(k) if along_x else y_peer(k)
        if phase == 0:
            ref = hg.at[h, y, x]
        elif along_x:
            ref = hg.at[h, :, x]
        else:
            ref = hg.at[h, y]
        return copy(ref, ref, head_send.at[h, phase, k], head_recv.at[h, phase, k], dev)

    def spread_in(h, phase, k):
        along_x = (h == 0) == (phase == 0)
        n = X if along_x else Y
        src_x = lax.rem(x + X - k, X)
        src_y = lax.rem(y + Y - k, Y)
        if phase == 0:
            ref = hg.at[h, y, src_x] if along_x else hg.at[h, src_y, x]
        elif along_x:
            ref = hg.at[h, :, src_x]
        else:
            ref = hg.at[h, src_y]
        return copy(ref, ref, head_send.at[h, phase, k], head_recv.at[h, phase, k], partner)

    def count(h, phase):
        return X if (h == 0) == (phase == 0) else Y

    for phase in range(2):
        for h in range(2):
            if phase == 1:
                for k in range(1, count(h, 0)):
                    spread_in(h, 0, k).wait_recv()
            for k in range(1, count(h, phase)):
                spread(h, phase, k).start()
        if phase == 0:
            combine()
        else:
            finish()

    for h in range(2):
        for k in range(1, count(h, 1)):
            spread_in(h, 1, k).wait_recv()
        heads = X * Y
        flat = hg.at[h]
        total = jnp.zeros((quarter, 256), jnp.float32)
        for pair in range(heads // 2):
            a, b = 2 * pair, 2 * pair + 1
            lhs = jnp.concatenate([flat[a // X, a % X], flat[b // X, b % X]], axis=1)
            total = total + jnp.dot(lhs, wb[pair * 256:(pair + 1) * 256, :],
                                    preferred_element_type=jnp.float32)
        out_ref[h * quarter:(h + 1) * quarter, :] = total[:, 0:128].astype(jnp.bfloat16)
        out_ref[half + h * quarter:half + (h + 1) * quarter, :] = total[:, 128:256].astype(jnp.bfloat16)

    for c in range(NCH):
        @pl.when(z < Z - 1)
        def _():
            first(c, 1, up).wait_send()

        @pl.when(z < ND)
        def _():
            first(c, NU + 1, down).wait_send()

        first_pair(c).wait_send()

    def drain(s, _):
        for c in range(NCH):
            @pl.when(s <= z)
            def _():
                to_pair(s, c).wait_send()

                @pl.when(jnp.logical_and(s < NU, z < Z - 1))
                def _():
                    onward(s, c, up).wait_send()

            @pl.when(jnp.logical_and(s <= ND, lax.rem(z + s, Z) < ND))
            def _():
                @pl.when(s < ND)
                def _():
                    onward(NU + s, c, down).wait_send()

                @pl.when(z + s >= Z)
                def _():
                    to_pair(NU + s, c).wait_send()
        return 0

    lax.fori_loop(1, NU + 1, drain, 0)
    drain_experts()
    for phase in range(2):
        for h in range(2):
            for k in range(1, count(h, phase)):
                spread(h, phase, k).wait_send()


def dot_nn(a, b):
    return jnp.dot(a, b, preferred_element_type=jnp.float32)


def dot_nt(a, b):
    return lax.dot_general(a, b, (((1,), (1,)), ((), ())), preferred_element_type=jnp.float32)


def dot_tn(a, b):
    return lax.dot_general(a, b, (((0,), (0,)), ((), ())), preferred_element_type=jnp.float32)


def iota(shape, dim):
    return lax.broadcasted_iota(jnp.int32, shape, dim)


def as_bf16(flags):
    return jnp.where(flags, 1.0, 0.0).astype(jnp.bfloat16)


def expert_stages(dims, copy, x_peer, y_peer, ins, out_ref, scratch):
    n_ep, Y, X, T = dims
    x_in, gain_in, routes_in, share_in, gate_in, up_in, down_in, sgate_in, sup_in, sdown_in = ins
    (normed, ob, rb, fa, gw, uw, dw, ha, ro, cb, ps, pr, sh, mix, mix_end,
     z_sems, w_sems, y_sems, p_sems, s_sems) = scratch
    ep = lax.axis_index("ep")
    tp = lax.axis_index("tp")
    y, x = tp // X, tp % X
    D = normed.shape[1]
    DY = D // Y
    B8 = 8 * n_ep
    HU = gate_in.shape[1]

    def ep_peer(k):
        return (lax.rem(ep + k, n_ep), tp)

    def ep_from(k):
        return lax.rem(ep + n_ep - k, n_ep)

    def x_to(k):
        return lax.rem(x + k, X)

    def x_from(k):
        return lax.rem(x + X - k, X)

    def y_from(k):
        return lax.rem(y + Y - k, Y)

    def weight_copies(k, incoming):
        to, place = x_to(k), (x_from(k) if incoming else x)
        rows = pl.ds(pl.multiple_of(place * HU, HU), HU)
        return [
            copy(gate_in.at[to], gw.at[rows], w_sems.at[0, 0, k], w_sems.at[1, 0, k], x_peer(k)),
            copy(up_in.at[to], uw.at[rows], w_sems.at[0, 1, k], w_sems.at[1, 1, k], x_peer(k)),
            copy(down_in.at[to], dw.at[place], w_sems.at[0, 2, k], w_sems.at[1, 2, k], x_peer(k)),
        ]

    def keep_weights():
        rows = pl.ds(pl.multiple_of(x * HU, HU), HU)
        gw[rows, :] = gate_in[x]
        uw[rows, :] = up_in[x]
        dw[x] = down_in[x]

    def send_weights():
        for k in range(1, X):
            for c in weight_copies(k, False):
                c.start()

    def out_copy(k):
        to = lax.rem(ep + k, n_ep)
        return copy(ob.at[to], rb.at[ep], z_sems.at[0, 0, k], z_sems.at[0, 1, k], ep_peer(k))

    def in_copy(k):
        return copy(ob.at[ep], rb.at[ep_from(k)], z_sems.at[0, 0, k], z_sems.at[0, 1, k], ep_peer(k))

    def back_copy(k):
        to = lax.rem(ep + k, n_ep)
        return copy(ro.at[to], cb.at[ep], z_sems.at[1, 0, k], z_sems.at[1, 1, k], ep_peer(k))

    def returned_copy(k):
        return copy(ro.at[ep], cb.at[ep_from(k)], z_sems.at[1, 0, k], z_sems.at[1, 1, k], ep_peer(k))

    def each(first, last, fn):
        def body(k, carry):
            fn(k)
            return carry
        lax.fori_loop(first, last, body, 0)

    def row_copy(k):
        return copy(fa.at[y], fa.at[y], y_sems.at[0, 0, k], y_sems.at[0, 1, k], y_peer(k))

    def row_in(k):
        return copy(fa.at[y], fa.at[y_from(k)], y_sems.at[0, 0, k], y_sems.at[0, 1, k], y_peer(k))

    def hid_copy(k):
        return copy(ha.at[y], ha.at[y], y_sems.at[1, 0, k], y_sems.at[1, 1, k], y_peer(k))

    def hid_in(k):
        return copy(ha.at[y], ha.at[y_from(k)], y_sems.at[1, 0, k], y_sems.at[1, 1, k], y_peer(k))

    def part_copy(k):
        return copy(ps.at[x_to(k)], pr.at[x], p_sems.at[0, k], p_sems.at[1, k], x_peer(k))

    def part_in(k):
        return copy(ps.at[x], pr.at[x_from(k)], p_sems.at[0, k], p_sems.at[1, k], x_peer(k))

    def share_x(k):
        return copy(sh.at[y, x], sh.at[y, x], s_sems.at[0, 0, k], s_sems.at[0, 1, k], x_peer(k))

    def share_x_in(k):
        return copy(sh.at[y, x], sh.at[y, x_from(k)], s_sems.at[0, 0, k], s_sems.at[0, 1, k], x_peer(k))

    def share_y(k):
        return copy(sh.at[y], sh.at[y], s_sems.at[1, 0, k], s_sems.at[1, 1, k], y_peer(k))

    def share_y_in(k):
        return copy(sh.at[y], sh.at[y_from(k)], s_sems.at[1, 0, k], s_sems.at[1, 1, k], y_peer(k))

    def pick(wide):
        row = iota((B8, 128), 0) % 8
        total = jnp.zeros((B8, 128), jnp.float32)
        for c in range(X):
            total = total + jnp.where(row == c, wide[:, c * 128:(c + 1) * 128], 0.0)
        return total

    def to_tiles(value):
        return value.reshape(n_ep, 8, 128).astype(jnp.bfloat16)

    def from_tiles(tiles):
        return tiles.astype(jnp.float32).reshape(B8, 128).astype(jnp.bfloat16)

    def ninth(tile, c):
        chosen = as_bf16(iota((n_ep, B8), 1) == 8 * iota((n_ep, B8), 0) + c)
        return dot_nn(chosen, tile)

    def spread_rows(value):
        expand = as_bf16(iota((B8, n_ep), 0) // 8 == iota((B8, n_ep), 1))
        return dot_nn(expand, value)

    def dispatch():
        rows = x_in[...].astype(jnp.float32)
        mean = jnp.mean(rows * rows, axis=1, keepdims=True)
        normed[...] = (rows * lax.rsqrt(mean + norm_eps) * gain_in[...]).astype(jnp.bfloat16)
        named = iota((n_ep, T), 0) * X + x
        hit = jnp.zeros((n_ep, T), jnp.float32)
        weight = jnp.zeros((n_ep, T), jnp.float32)
        for j in range(TOP):
            same = named == routes_in[j:j + 1, :]
            hit = hit + jnp.where(same, 1.0, 0.0)
            weight = weight + jnp.where(same, share_in[j:j + 1, :], 0.0)
        before = as_bf16(iota((T, T), 0) < iota((T, T), 1))
        rank = jnp.where(hit > 0.0, dot_nn(hit.astype(jnp.bfloat16), before), -1.0)
        place = spread_rows(rank.astype(jnp.bfloat16))
        mine = normed[:, pl.ds(pl.multiple_of(y * DY, 128), DY)]
        slot = (iota((B8, T), 0) % 8).astype(jnp.float32)
        main = dot_nn(as_bf16(place == slot), mine)
        last = pick(dot_nn(as_bf16(place == 8.0), mine))
        for c in range(X):
            ob[:, c] = to_tiles(main[:, c * 128:(c + 1) * 128])
        ob[:, X] = to_tiles(last)
        rb[ep] = ob[ep]
        high = weight.astype(jnp.bfloat16)
        low = (weight - high.astype(jnp.float32)).astype(jnp.bfloat16)
        for n, piece in enumerate((high, low)):
            mix[n] = jnp.where(place == slot, spread_rows(piece), 0.0).astype(jnp.bfloat16)
            mix_end[n] = jnp.where(rank == 8.0, piece.astype(jnp.float32), 0.0).astype(jnp.bfloat16)

    def send_rows():
        each(1, n_ep, lambda k: out_copy(k).start())

    def shared_first():
        gate = dot_nt(sgate_in[...], normed[...])
        up = dot_nt(sup_in[...], normed[...])
        sh[y, x] = (gate / (1.0 + jnp.exp(-gate)) * up).astype(jnp.bfloat16)

    def send_shared():
        for k in range(1, X):
            share_x(k).start()

    def shared_second():
        for k in range(1, X):
            share_x_in(k).wait_recv()
        for k in range(1, Y):
            share_y(k).start()

    def gather_rows():
        each(1, n_ep, lambda k: in_copy(k).wait_recv())
        tile = from_tiles(rb[:, X])
        for c in range(X):
            fa[y, 0:B8, c * 128:(c + 1) * 128] = from_tiles(rb[:, c])
            fa[y, B8:B8 + n_ep, c * 128:(c + 1) * 128] = ninth(tile, c).astype(jnp.bfloat16)
        for k in range(1, Y):
            row_copy(k).start()

    def first_products():
        for k in range(1, X):
            for c in weight_copies(k, True):
                c.wait_recv()
        for k in range(1, Y):
            row_in(k).wait_recv()
        gate = jnp.zeros((B8 + n_ep, X * HU), jnp.float32)
        up = jnp.zeros((B8 + n_ep, X * HU), jnp.float32)
        for part in range(Y):
            piece = fa[part]
            gate = gate + dot_nt(piece, gw[:, part * DY:(part + 1) * DY])
            up = up + dot_nt(piece, uw[:, part * DY:(part + 1) * DY])
        ha[y] = (gate / (1.0 + jnp.exp(-gate)) * up).astype(jnp.bfloat16)
        for k in range(1, Y):
            hid_copy(k).start()

    def second_products():
        for k in range(1, Y):
            hid_in(k).wait_recv()
        hidden = jnp.concatenate([ha[part] for part in range(Y)], axis=1)
        ends = []
        for c in range(X):
            result = dot_nn(hidden, dw[c])
            ro[:, c] = to_tiles(result[0:B8])
            ends.append(result[B8:B8 + n_ep].astype(jnp.bfloat16))
        ro[:, X] = to_tiles(pick(spread_rows(jnp.concatenate(ends, axis=1))))
        each(1, n_ep, lambda k: back_copy(k).start())
        cb[ep] = ro[ep]

    def combine():
        each(1, n_ep, lambda k: returned_copy(k).wait_recv())
        main = jnp.concatenate([from_tiles(cb[:, c]) for c in range(X)], axis=1)
        tile = from_tiles(cb[:, X])
        last = jnp.concatenate([ninth(tile, c).astype(jnp.bfloat16) for c in range(X)], axis=1)
        total = jnp.zeros((T, DY), jnp.float32)
        for n in range(2):
            total = total + dot_tn(mix[n], main) + dot_tn(mix_end[n], last)
        for c in range(X):
            ps[c] = total[:, c * 128:(c + 1) * 128]
        for k in range(1, X):
            part_copy(k).start()

    def finish():
        for k in range(1, Y):
            share_y_in(k).wait_recv()
        hidden = jnp.concatenate([sh[a, b] for a in range(Y) for b in range(X)], axis=0)
        total = dot_tn(hidden, sdown_in[...])
        for k in range(1, X):
            part_in(k).wait_recv()
        total = total + ps[x]
        for k in range(1, X):
            total = total + pr[x_from(k)]
        out_ref[...] = total.astype(jnp.bfloat16)

    def drain():
        each(1, n_ep, lambda k: out_copy(k).wait_send())
        each(1, n_ep, lambda k: back_copy(k).wait_send())
        for k in range(1, X):
            for c in weight_copies(k, False):
                c.wait_send()
            share_x(k).wait_send()
            part_copy(k).wait_send()
        for k in range(1, Y):
            share_y(k).wait_send()
            row_copy(k).wait_send()
            hid_copy(k).wait_send()

    return (keep_weights, send_weights, dispatch, send_rows, shared_first, send_shared, shared_second,
            gather_rows, first_products, second_products, combine, finish, drain)


def expert_scratch(n_ep, Y, X, T, D, HU, FF):
    B8 = 8 * n_ep
    tiles = (n_ep, X + 1, 8, 128)
    bf16 = jnp.bfloat16
    return [
        pltpu.VMEM((T, D), bf16),
        pltpu.VMEM(tiles, bf16),
        pltpu.VMEM(tiles, bf16),
        pltpu.VMEM((Y, B8 + n_ep, D // Y), bf16),
        pltpu.VMEM((X * HU, D), bf16),
        pltpu.VMEM((X * HU, D), bf16),
        pltpu.VMEM((X, FF, 128), bf16),
        pltpu.VMEM((Y, B8 + n_ep, X * HU), bf16),
        pltpu.VMEM(tiles, bf16),
        pltpu.VMEM(tiles, bf16),
        pltpu.VMEM((X, T, 128), jnp.float32),
        pltpu.VMEM((X, T, 128), jnp.float32),
        pltpu.VMEM((Y, X, HU, T), bf16),
        pltpu.VMEM((2, B8, T), bf16),
        pltpu.VMEM((2, n_ep, T), bf16),
        pltpu.SemaphoreType.DMA((2, 2, n_ep)),
        pltpu.SemaphoreType.DMA((2, 3, X)),
        pltpu.SemaphoreType.DMA((2, 2, Y)),
        pltpu.SemaphoreType.DMA((2, X)),
        pltpu.SemaphoreType.DMA((2, 2, 4)),
    ]


def local(
    query_rows,
    key_rows,
    value_rows,
    cum_gate,
    out_weight,
    moe_input,
    moe_gain,
    routes,
    route_weight,
    expert_gate,
    expert_up,
    expert_down,
    shared_gate,
    shared_up,
    shared_down,
):
    n_ep, n_tp = lax.axis_size("ep"), lax.axis_size("tp")
    X = expert_gate.shape[0]
    Y = n_tp // X
    Z = n_ep // 2
    R = query_rows.shape[0]
    CH = 256
    T, D = moe_input.shape
    HU = expert_gate.shape[2]
    vm = pl.BlockSpec(memory_space=pltpu.VMEM)
    step = pl.pallas_call(
        functools.partial(step_kernel, (Z, Y, X, R, CH), STOPS),
        out_shape=(
            jax.ShapeDtypeStruct((R, out_weight.shape[1]), jnp.bfloat16),
            jax.ShapeDtypeStruct((T, out_weight.shape[1]), jnp.bfloat16),
        ),
        in_specs=[vm] * 15,
        out_specs=(vm, vm),
        scratch_shapes=[
            pltpu.VMEM((Z, R // CH, 2, 2 * HEAD, CH), jnp.bfloat16),
            pltpu.VMEM((R, 256), jnp.bfloat16),
            pltpu.VMEM((R, 128), jnp.float32),
            pltpu.VMEM((R, 128), jnp.float32),
            pltpu.VMEM((2, Y, X, R // 4, 128), jnp.bfloat16),
            pltpu.VMEM((n_tp * 128, 256), jnp.bfloat16),
            pltpu.SemaphoreType.DMA((Z, R // CH)),
            pltpu.SemaphoreType.DMA((Z, R // CH)),
            pltpu.SemaphoreType.DMA((Z, R // CH)),
            pltpu.SemaphoreType.DMA((Z, R // CH)),
            pltpu.SemaphoreType.DMA((2, 2, 4)),
            pltpu.SemaphoreType.DMA((2, 2, 4)),
        ]
        + expert_scratch(n_ep, Y, X, T, D, HU, expert_down.shape[1]),
        compiler_params=pltpu.CompilerParams(
            collective_id=0, has_side_effects=True, vmem_limit_bytes=56 * 1024 * 1024
        ),
    )
    return step(
        query_rows.T,
        key_rows.T,
        value_rows.T,
        cum_gate,
        out_weight,
        moe_input,
        moe_gain[None, :],
        routes.T,
        route_weight.T,
        expert_gate.swapaxes(1, 2),
        expert_up.swapaxes(1, 2),
        expert_down,
        shared_gate.T,
        shared_up.T,
        shared_down,
    )


def solution(mesh):
    placed = (
        P("ep", "tp"),
        P("ep", "tp"),
        P("ep", "tp"),
        P("tp", None),
        P(None, "tp"),
        P("ep", None),
        P(),
        P("ep", None),
        P("ep", None),
        P("ep", None, "tp"),
        P("ep", None, "tp"),
        P("ep", None, "tp"),
        P(None, "tp"),
        P(None, "tp"),
        P(None, "tp"),
    )
    return jax.shard_map(
        local, mesh=mesh, in_specs=placed, out_specs=(P("ep", "tp"), P("ep", "tp")), check_vma=False
    )
```

```python
import functools
import jax
import jax.numpy as jnp
from jax import lax
from jax.experimental import pallas as pl
from jax.experimental.pallas import tpu as pltpu
from jax.sharding import PartitionSpec as P

HEAD = 64
TOP = 3
LOG2E = 1.4426950408889634
MESH = pl.DeviceIdType.MESH
STOPS = (2, 4, 9, 10, 12, 15, 18)
neg_fill = -1e30
norm_eps = 1e-06


def in_three(value):
    hi = value.astype(jnp.bfloat16)
    left = value - hi.astype(jnp.float32)
    mid = left.astype(jnp.bfloat16)
    low = (left - mid.astype(jnp.float32)).astype(jnp.bfloat16)
    return hi, mid, low


def step_kernel(dims, stops, *refs):
    qT_ref, kT_ref, vT_ref, cg_ref, w_ref = refs[0:5]
    expert_ins = refs[5:15]
    out_ref, moe_ref = refs[15:17]
    kv, qs, acc, mx, hg, wb, ring_send, ring_recv, pair_send, pair_recv, head_send, head_recv = refs[17:29]
    expert_scratch_refs = refs[29:]
    Z, Y, X, R, CH = dims
    NCH = R // CH
    QT = R // 256
    NU, ND = Z // 2, Z // 2 - 1
    ep = lax.axis_index("ep")
    tp = lax.axis_index("tp")
    z, core = ep // 2, ep % 2
    y, x = tp // X, tp % X
    up = (lax.rem(ep + 2, 2 * Z), tp)
    down = (lax.rem(ep + 2 * Z - 2, 2 * Z), tp)
    partner = (2 * z + 1 - core, tp)

    def x_peer(k):
        return (ep, y * X + lax.rem(x + k, X))

    def y_peer(k):
        return (ep, lax.rem(y + k, Y) * X + x)

    barrier = pltpu.get_barrier_semaphore()
    peers = [x_peer(k) for k in range(1, X)] + [y_peer(k) for k in range(1, Y)]
    for peer in peers:
        pl.semaphore_signal(barrier, inc=1, device_id=peer, device_id_type=MESH)

    def greet(k, carry):
        pl.semaphore_signal(barrier, inc=1, device_id=(lax.rem(ep + k, 2 * Z), tp), device_id_type=MESH)
        return carry

    lax.fori_loop(1, 2 * Z, greet, 0)

    def copy(src, dst, ssem, rsem, dev):
        return pltpu.make_async_remote_copy(
            src_ref=src, dst_ref=dst, send_sem=ssem, recv_sem=rsem,
            device_id=dev, device_id_type=MESH)

    def halves(c, target, ssem, rsem, dev):
        keys = copy(kT_ref.at[:, pl.ds(c * CH, CH)], target.at[0:HEAD], ssem, rsem, dev)
        values = copy(vT_ref.at[:, pl.ds(c * CH, CH)], target.at[HEAD:2 * HEAD], ssem, rsem, dev)
        keys.start()
        values.start()

    def start_first(c, slot, dev):
        halves(c, kv.at[slot, c, 0], ring_send.at[slot, c], ring_recv.at[slot, c], dev)

    def start_first_pair(c):
        halves(c, kv.at[0, c, 1], pair_send.at[0, c], pair_recv.at[0, c], partner)

    def first(c, slot, dev):
        return copy(kv.at[slot, c, 0], kv.at[slot, c, 0], ring_send.at[slot, c], ring_recv.at[slot, c], dev)

    def first_pair(c):
        return copy(kv.at[0, c, 1], kv.at[0, c, 1], pair_send.at[0, c], pair_recv.at[0, c], partner)

    def onward(slot, c, dev):
        return copy(kv.at[slot, c, 0], kv.at[slot + 1, c, 0],
                    ring_send.at[slot + 1, c], ring_recv.at[slot + 1, c], dev)

    def to_pair(slot, c):
        return copy(kv.at[slot, c, 0], kv.at[slot, c, 1],
                    pair_send.at[slot, c], pair_recv.at[slot, c], partner)

    (keep_weights, send_weights, dispatch, send_rows, shared_first, send_shared, shared_second,
     gather_rows, first_products, second_products, combine, finish, drain_experts) = expert_stages(
        (2 * Z, Y, X, expert_ins[0].shape[0]), copy, x_peer, y_peer, expert_ins, moe_ref, expert_scratch_refs)

    dispatch()
    shared_first()
    keep_weights()
    q_all = jnp.transpose(qT_ref[...].astype(jnp.float32)) * (HEAD ** -0.5 * LOG2E)
    q_hi, q_mid, q_lo = in_three(q_all)
    q_one = jnp.where(lax.broadcasted_iota(jnp.int32, (R, HEAD), 1) < 3, 1.0, 0.0).astype(jnp.bfloat16)
    qs[:, 0:128] = jnp.concatenate([q_hi, q_mid], axis=1)
    qs[:, 128:256] = jnp.concatenate([q_lo, q_one], axis=1)
    mx[...] = jnp.full(mx.shape, neg_fill, jnp.float32)
    acc[...] = jnp.zeros(acc.shape, jnp.float32)
    wb[...] = jnp.zeros(wb.shape, jnp.bfloat16)

    def place(h, _):
        part = w_ref[pl.ds(pl.multiple_of(h * HEAD, HEAD), HEAD), :]
        wb[pl.ds(pl.multiple_of(h * 128, 128), HEAD), 0:128] = part
        wb[pl.ds(pl.multiple_of(h * 128 + HEAD, HEAD), HEAD), 128:256] = part
        return 0

    lax.fori_loop(0, w_ref.shape[0] // HEAD, place, 0)

    first_row = pl.multiple_of(ep * R, 128)
    base_gate = cg_ref[:, pl.ds(first_row, 128)][:, 0:1]

    def gate_of(block, c):
        at = pl.multiple_of(block * R + c * CH, 128)
        return (base_gate - cg_ref[:, pl.ds(at, CH)]) * LOG2E

    def score_side(pair, gate):
        hi, mid, lo = in_three(gate)
        row = lax.broadcasted_iota(jnp.int32, (HEAD, CH), 0)
        hi, mid, lo = (piece.astype(jnp.float32) for piece in (hi, mid, lo))
        gates = jnp.where(row == 0, hi, jnp.where(row == 1, mid, jnp.where(row == 2, lo, 0.0)))
        keys = pair[0:HEAD, :]
        return jnp.concatenate([keys, keys, keys, gates.astype(jnp.bfloat16)], axis=0)

    def value_side(pair):
        return jnp.concatenate([jnp.ones((HEAD, CH), jnp.bfloat16), pair[HEAD:2 * HEAD, :]], axis=0)

    def update(i, sides, masked=False):
        rows = slice(i * 256, (i + 1) * 256)
        q = qs[rows, :]
        logits = [jnp.dot(q, keys, preferred_element_type=jnp.float32) for keys, _ in sides]
        if masked:
            qi = lax.broadcasted_iota(jnp.int32, logits[0].shape, 0)
            ki = lax.broadcasted_iota(jnp.int32, logits[0].shape, 1)
            logits[0] = jnp.where(ki <= qi, logits[0], neg_fill)
        tops = [s[:, at:at + 128] for s in logits for at in range(0, CH, 128)]
        top = tops[0]
        for s in tops[1:]:
            top = jnp.maximum(top, s)
        old = mx[rows, :]
        new = jnp.maximum(old, jnp.max(top, axis=1, keepdims=True))
        wide = jnp.concatenate([new] * (CH // 128), axis=1)
        total = acc[rows, :] * jnp.exp2(old - new)
        for s, (_, values) in zip(logits, sides):
            p = jnp.exp2(s - wide).astype(jnp.bfloat16)
            total = total + lax.dot_general(
                p, values, (((1,), (1,)), ((), ())), preferred_element_type=jnp.float32)
        acc[rows, :] = total
        mx[rows, :] = new

    def sides_of(pair, block, c):
        return score_side(pair, gate_of(block, c)), value_side(pair)

    for c in range(NCH):
        side = sides_of(jnp.concatenate([kT_ref[:, c * CH:(c + 1) * CH], vT_ref[:, c * CH:(c + 1) * CH]], axis=0), ep, c)
        for i in range(c, QT):
            update(i, [side], i == c)

    pl.semaphore_wait(barrier, len(peers) + 2 * Z - 1)
    for c in range(NCH):
        @pl.when(z < Z - 1)
        def _():
            start_first(c, 1, up)

        @pl.when(z < ND)
        def _():
            start_first(c, NU + 1, down)

        start_first_pair(c)

    send_rows()
    send_weights()
    send_shared()
    for c in range(NCH):
        first_pair(c).wait_recv()

    @pl.when(core == 1)
    def _():
        for c in range(NCH):
            side = sides_of(kv[0, c, 1], ep - 1, c)
            for i in range(QT):
                update(i, [side])

    def issue(s, c):
        @pl.when(s <= z)
        def _():
            onward(s - 1, c, up).wait_recv()
            to_pair(s, c).start()

            @pl.when(jnp.logical_and(s < NU, z < Z - 1))
            def _():
                onward(s, c, up).start()

        @pl.when(jnp.logical_and(s <= ND, lax.rem(z + s, Z) < ND))
        def _():
            onward(NU + s - 1, c, down).wait_recv()

            @pl.when(s < ND)
            def _():
                onward(NU + s, c, down).start()

            @pl.when(z + s >= Z)
            def _():
                to_pair(NU + s, c).start()

    def attend(slot, c, chip):
        sides = [sides_of(kv[slot, c, 0], 2 * chip + core, c), sides_of(kv[slot, c, 1], 2 * chip + 1 - core, c)]
        for i in range(QT):
            update(i, sides)

    def consume(s, c):
        @pl.when(s <= z)
        def _():
            to_pair(s, c).wait_recv()
            attend(s, c, z - s)

        @pl.when(jnp.logical_and(s <= ND, z + s >= Z))
        def _():
            to_pair(NU + s, c).wait_recv()
            attend(NU + s, c, z + s - Z)

    steps = NU * NCH

    def step(t, _):
        @pl.when(t < steps)
        def _():
            issue(t // NCH + 1, t % NCH)

        for at, stage in zip(stops, (
            shared_second,
            lambda: gather_rows(0), lambda: first_products(0), lambda: gather_rows(1),
            lambda: second_products(0), lambda: first_products(1), lambda: second_products(1))):
            @pl.when(t == at)
            def _():
                stage()

        @pl.when(t >= 1)
        def _():
            consume((t - 1) // NCH + 1, (t - 1) % NCH)

        return 0

    lax.fori_loop(0, steps + 1, step, 0)

    quarter, half = R // 4, R // 2
    low = lax.broadcasted_iota(jnp.int32, (quarter, 128), 1) < HEAD

    def finished(at):
        a = acc[at:at + quarter, :]
        return a / pltpu.roll(a, HEAD, 1)

    for h in range(2):
        first_half = pltpu.roll(finished(h * quarter), HEAD, 1)
        second_half = finished(half + h * quarter)
        hg[h, y, x] = jnp.where(low, first_half, second_half).astype(jnp.bfloat16)

    def spread(h, phase, k):
        along_x = (h == 0) == (phase == 0)
        dev = x_peer(k) if along_x else y_peer(k)
        if phase == 0:
            ref = hg.at[h, y, x]
        elif along_x:
            ref = hg.at[h, :, x]
        else:
            ref = hg.at[h, y]
        return copy(ref, ref, head_send.at[h, phase, k], head_recv.at[h, phase, k], dev)

    def spread_in(h, phase, k):
        along_x = (h == 0) == (phase == 0)
        n = X if along_x else Y
        src_x = lax.rem(x + X - k, X)
        src_y = lax.rem(y + Y - k, Y)
        if phase == 0:
            ref = hg.at[h, y, src_x] if along_x else hg.at[h, src_y, x]
        elif along_x:
            ref = hg.at[h, :, src_x]
        else:
            ref = hg.at[h, src_y]
        return copy(ref, ref, head_send.at[h, phase, k], head_recv.at[h, phase, k], partner)

    def count(h, phase):
        return X if (h == 0) == (phase == 0) else Y

    for phase in range(2):
        for h in range(2):
            if phase == 1:
                for k in range(1, count(h, 0)):
                    spread_in(h, 0, k).wait_recv()
            for k in range(1, count(h, phase)):
                spread(h, phase, k).start()
        if phase == 0:
            combine()
        else:
            finish()

    for h in range(2):
        for k in range(1, count(h, 1)):
            spread_in(h, 1, k).wait_recv()
        heads = X * Y
        flat = hg.at[h]
        total = jnp.zeros((quarter, 256), jnp.float32)
        for pair in range(heads // 2):
            a, b = 2 * pair, 2 * pair + 1
            lhs = jnp.concatenate([flat[a // X, a % X], flat[b // X, b % X]], axis=1)
            total = total + jnp.dot(lhs, wb[pair * 256:(pair + 1) * 256, :],
                                    preferred_element_type=jnp.float32)
        out_ref[h * quarter:(h + 1) * quarter, :] = total[:, 0:128].astype(jnp.bfloat16)
        out_ref[half + h * quarter:half + (h + 1) * quarter, :] = total[:, 128:256].astype(jnp.bfloat16)

    for c in range(NCH):
        @pl.when(z < Z - 1)
        def _():
            first(c, 1, up).wait_send()

        @pl.when(z < ND)
        def _():
            first(c, NU + 1, down).wait_send()

        first_pair(c).wait_send()

    def drain(s, _):
        for c in range(NCH):
            @pl.when(s <= z)
            def _():
                to_pair(s, c).wait_send()

                @pl.when(jnp.logical_and(s < NU, z < Z - 1))
                def _():
                    onward(s, c, up).wait_send()

            @pl.when(jnp.logical_and(s <= ND, lax.rem(z + s, Z) < ND))
            def _():
                @pl.when(s < ND)
                def _():
                    onward(NU + s, c, down).wait_send()

                @pl.when(z + s >= Z)
                def _():
                    to_pair(NU + s, c).wait_send()
        return 0

    lax.fori_loop(1, NU + 1, drain, 0)
    drain_experts()
    for phase in range(2):
        for h in range(2):
            for k in range(1, count(h, phase)):
                spread(h, phase, k).wait_send()


def dot_nn(a, b):
    return jnp.dot(a, b, preferred_element_type=jnp.float32)


def dot_nt(a, b):
    return lax.dot_general(a, b, (((1,), (1,)), ((), ())), preferred_element_type=jnp.float32)


def dot_tn(a, b):
    return lax.dot_general(a, b, (((0,), (0,)), ((), ())), preferred_element_type=jnp.float32)


def iota(shape, dim):
    return lax.broadcasted_iota(jnp.int32, shape, dim)


def as_bf16(flags):
    return jnp.where(flags, 1.0, 0.0).astype(jnp.bfloat16)


def expert_stages(dims, copy, x_peer, y_peer, ins, out_ref, scratch):
    n_ep, Y, X, T = dims
    x_in, gain_in, routes_in, share_in, gate_in, up_in, down_in, sgate_in, sup_in, sdown_in = ins
    (normed, ob, rb, fa, gw, uw, dw, ha, ro, cb, ps, pr, sh, mix, mix_end,
     z_sems, w_sems, y_sems, p_sems, s_sems) = scratch
    ep = lax.axis_index("ep")
    tp = lax.axis_index("tp")
    y, x = tp // X, tp % X
    D = normed.shape[1]
    DY = D // Y
    B8 = 8 * n_ep
    quart, nh, bh = n_ep // 4, n_ep // 2, 4 * n_ep
    HU = gate_in.shape[1]

    def ep_peer(k):
        return (lax.rem(ep + k, n_ep), tp)

    def ep_from(k):
        return lax.rem(ep + n_ep - k, n_ep)

    def x_to(k):
        return lax.rem(x + k, X)

    def x_from(k):
        return lax.rem(x + X - k, X)

    def y_from(k):
        return lax.rem(y + Y - k, Y)

    def weight_copies(k, incoming):
        to, place = x_to(k), (x_from(k) if incoming else x)
        rows = pl.ds(pl.multiple_of(place * HU, HU), HU)
        return [
            copy(gate_in.at[to], gw.at[rows], w_sems.at[0, 0, k], w_sems.at[1, 0, k], x_peer(k)),
            copy(up_in.at[to], uw.at[rows], w_sems.at[0, 1, k], w_sems.at[1, 1, k], x_peer(k)),
            copy(down_in.at[to], dw.at[place], w_sems.at[0, 2, k], w_sems.at[1, 2, k], x_peer(k)),
        ]

    def keep_weights():
        rows = pl.ds(pl.multiple_of(x * HU, HU), HU)
        gw[rows, :] = gate_in[x]
        uw[rows, :] = up_in[x]
        dw[x] = down_in[x]

    def send_weights():
        for k in range(1, X):
            for c in weight_copies(k, False):
                c.start()

    def place_of(k):
        return lax.rem(k + quart, n_ep)

    def group_each(g, fn):
        if g == 0:
            each(1, quart, fn)
            each(n_ep - quart, n_ep, fn)
        else:
            each(quart, n_ep - quart, fn)

    def out_copy(k):
        to = lax.rem(ep + k, n_ep)
        return copy(ob.at[to], rb.at[place_of(k)], z_sems.at[0, 0, k], z_sems.at[0, 1, k], ep_peer(k))

    def in_copy(k):
        return copy(ob.at[ep], rb.at[place_of(k)], z_sems.at[0, 0, k], z_sems.at[0, 1, k], ep_peer(k))

    def back_copy(k):
        return copy(ro.at[place_of(k)], cb.at[ep], z_sems.at[1, 0, k], z_sems.at[1, 1, k], (ep_from(k), tp))

    def returned_copy(k):
        return copy(ro.at[0], cb.at[lax.rem(ep + k, n_ep)], z_sems.at[1, 0, k], z_sems.at[1, 1, k], ep_peer(k))

    def each(first, last, fn):
        def body(k, carry):
            fn(k)
            return carry
        lax.fori_loop(first, last, body, 0)

    def row_copy(g, k):
        return copy(fa.at[g, y], fa.at[g, y], y_sems.at[g, 0, 0, k], y_sems.at[g, 0, 1, k], y_peer(k))

    def row_in(g, k):
        return copy(fa.at[g, y], fa.at[g, y_from(k)], y_sems.at[g, 0, 0, k], y_sems.at[g, 0, 1, k], y_peer(k))

    def hid_copy(g, k):
        return copy(ha.at[g, y], ha.at[g, y], y_sems.at[g, 1, 0, k], y_sems.at[g, 1, 1, k], y_peer(k))

    def hid_in(g, k):
        return copy(ha.at[g, y], ha.at[g, y_from(k)], y_sems.at[g, 1, 0, k], y_sems.at[g, 1, 1, k], y_peer(k))

    def part_copy(k):
        return copy(ps.at[x_to(k)], pr.at[x], p_sems.at[0, k], p_sems.at[1, k], x_peer(k))

    def part_in(k):
        return copy(ps.at[x], pr.at[x_from(k)], p_sems.at[0, k], p_sems.at[1, k], x_peer(k))

    def share_x(k):
        return copy(sh.at[y, x], sh.at[y, x], s_sems.at[0, 0, k], s_sems.at[0, 1, k], x_peer(k))

    def share_x_in(k):
        return copy(sh.at[y, x], sh.at[y, x_from(k)], s_sems.at[0, 0, k], s_sems.at[0, 1, k], x_peer(k))

    def share_y(k):
        return copy(sh.at[y], sh.at[y], s_sems.at[1, 0, k], s_sems.at[1, 1, k], y_peer(k))

    def share_y_in(k):
        return copy(sh.at[y], sh.at[y_from(k)], s_sems.at[1, 0, k], s_sems.at[1, 1, k], y_peer(k))

    def pick(wide):
        row = iota((wide.shape[0], 128), 0) % 8
        total = jnp.zeros((wide.shape[0], 128), jnp.float32)
        for c in range(X):
            total = total + jnp.where(row == c, wide[:, c * 128:(c + 1) * 128], 0.0)
        return total

    def to_tiles(value):
        return value.reshape(value.shape[0] // 8, 8, 128).astype(jnp.bfloat16)

    def from_tiles(tiles):
        return tiles.astype(jnp.float32).reshape(tiles.shape[0] * 8, 128).astype(jnp.bfloat16)

    def ninth(tile, c):
        n = tile.shape[0] // 8
        chosen = as_bf16(iota((n, 8 * n), 1) == 8 * iota((n, 8 * n), 0) + c)
        return dot_nn(chosen, tile)

    def spread_rows(value):
        n = value.shape[0]
        expand = as_bf16(iota((8 * n, n), 0) // 8 == iota((8 * n, n), 1))
        return dot_nn(expand, value)

    def dispatch():
        rows = x_in[...].astype(jnp.float32)
        mean = jnp.mean(rows * rows, axis=1, keepdims=True)
        normed[...] = (rows * lax.rsqrt(mean + norm_eps) * gain_in[...]).astype(jnp.bfloat16)
        named = iota((n_ep, T), 0) * X + x
        hit = jnp.zeros((n_ep, T), jnp.float32)
        weight = jnp.zeros((n_ep, T), jnp.float32)
        for j in range(TOP):
            same = named == routes_in[j:j + 1, :]
            hit = hit + jnp.where(same, 1.0, 0.0)
            weight = weight + jnp.where(same, share_in[j:j + 1, :], 0.0)
        before = as_bf16(iota((T, T), 0) < iota((T, T), 1))
        rank = jnp.where(hit > 0.0, dot_nn(hit.astype(jnp.bfloat16), before), -1.0)
        place = spread_rows(rank.astype(jnp.bfloat16))
        mine = normed[:, pl.ds(pl.multiple_of(y * DY, 128), DY)]
        slot = (iota((B8, T), 0) % 8).astype(jnp.float32)
        main = dot_nn(as_bf16(place == slot), mine)
        last = pick(dot_nn(as_bf16(place == 8.0), mine))
        for c in range(X):
            ob[:, c] = to_tiles(main[:, c * 128:(c + 1) * 128])
        ob[:, X] = to_tiles(last)
        rb[quart] = ob[ep]
        high = weight.astype(jnp.bfloat16)
        low = (weight - high.astype(jnp.float32)).astype(jnp.bfloat16)
        for n, piece in enumerate((high, low)):
            mix[n] = jnp.where(place == slot, spread_rows(piece), 0.0).astype(jnp.bfloat16)
            mix_end[n] = jnp.where(rank == 8.0, piece.astype(jnp.float32), 0.0).astype(jnp.bfloat16)

    def send_rows():
        for g in range(2):
            group_each(g, lambda k: out_copy(k).start())

    def shared_first():
        gate = dot_nt(sgate_in[...], normed[...])
        up = dot_nt(sup_in[...], normed[...])
        sh[y, x] = (gate / (1.0 + jnp.exp(-gate)) * up).astype(jnp.bfloat16)

    def send_shared():
        for k in range(1, X):
            share_x(k).start()

    def shared_second():
        for k in range(1, X):
            share_x_in(k).wait_recv()
        for k in range(1, Y):
            share_y(k).start()

    def gather_rows(g):
        group_each(g, lambda k: in_copy(k).wait_recv())
        span = slice(g * nh, (g + 1) * nh)
        tile = from_tiles(rb[span, X])
        for c in range(X):
            fa[g, y, 0:bh, c * 128:(c + 1) * 128] = from_tiles(rb[span, c])
            fa[g, y, bh:bh + nh, c * 128:(c + 1) * 128] = ninth(tile, c).astype(jnp.bfloat16)
        for k in range(1, Y):
            row_copy(g, k).start()

    def first_products(g):
        if g == 0:
            for k in range(1, X):
                for c in weight_copies(k, True):
                    c.wait_recv()
        for k in range(1, Y):
            row_in(g, k).wait_recv()
        gate = jnp.zeros((bh + nh, X * HU), jnp.float32)
        up = jnp.zeros((bh + nh, X * HU), jnp.float32)
        for part in range(Y):
            piece = fa[g, part]
            gate = gate + dot_nt(piece, gw[:, part * DY:(part + 1) * DY])
            up = up + dot_nt(piece, uw[:, part * DY:(part + 1) * DY])
        ha[g, y] = (gate / (1.0 + jnp.exp(-gate)) * up).astype(jnp.bfloat16)
        for k in range(1, Y):
            hid_copy(g, k).start()

    def second_products(g):
        for k in range(1, Y):
            hid_in(g, k).wait_recv()
        hidden = jnp.concatenate([ha[g, part] for part in range(Y)], axis=1)
        span = slice(g * nh, (g + 1) * nh)
        ends = []
        for c in range(X):
            result = dot_nn(hidden, dw[c])
            ro[span, c] = to_tiles(result[0:bh])
            ends.append(result[bh:bh + nh].astype(jnp.bfloat16))
        ro[span, X] = to_tiles(pick(spread_rows(jnp.concatenate(ends, axis=1))))
        group_each(g, lambda k: back_copy(k).start())
        if g == 0:
            cb[ep] = ro[quart]

    def combine():
        each(1, n_ep, lambda k: returned_copy(k).wait_recv())
        main = jnp.concatenate([from_tiles(cb[:, c]) for c in range(X)], axis=1)
        tile = from_tiles(cb[:, X])
        last = jnp.concatenate([ninth(tile, c).astype(jnp.bfloat16) for c in range(X)], axis=1)
        total = jnp.zeros((T, DY), jnp.float32)
        for n in range(2):
            total = total + dot_tn(mix[n], main) + dot_tn(mix_end[n], last)
        for c in range(X):
            ps[c] = total[:, c * 128:(c + 1) * 128]
        for k in range(1, X):
            part_copy(k).start()

    def finish():
        for k in range(1, Y):
            share_y_in(k).wait_recv()
        hidden = jnp.concatenate([sh[a, b] for a in range(Y) for b in range(X)], axis=0)
        total = dot_tn(hidden, sdown_in[...])
        for k in range(1, X):
            part_in(k).wait_recv()
        total = total + ps[x]
        for k in range(1, X):
            total = total + pr[x_from(k)]
        out_ref[...] = total.astype(jnp.bfloat16)

    def drain():
        each(1, n_ep, lambda k: out_copy(k).wait_send())
        each(1, n_ep, lambda k: back_copy(k).wait_send())
        for k in range(1, X):
            for c in weight_copies(k, False):
                c.wait_send()
            share_x(k).wait_send()
            part_copy(k).wait_send()
        for k in range(1, Y):
            share_y(k).wait_send()
            for g in range(2):
                row_copy(g, k).wait_send()
                hid_copy(g, k).wait_send()

    return (keep_weights, send_weights, dispatch, send_rows, shared_first, send_shared, shared_second,
            gather_rows, first_products, second_products, combine, finish, drain)


def expert_scratch(n_ep, Y, X, T, D, HU, FF):
    B8 = 8 * n_ep
    tiles = (n_ep, X + 1, 8, 128)
    bf16 = jnp.bfloat16
    return [
        pltpu.VMEM((T, D), bf16),
        pltpu.VMEM(tiles, bf16),
        pltpu.VMEM(tiles, bf16),
        pltpu.VMEM((2, Y, (B8 + n_ep) // 2, D // Y), bf16),
        pltpu.VMEM((X * HU, D), bf16),
        pltpu.VMEM((X * HU, D), bf16),
        pltpu.VMEM((X, FF, 128), bf16),
        pltpu.VMEM((2, Y, (B8 + n_ep) // 2, X * HU), bf16),
        pltpu.VMEM(tiles, bf16),
        pltpu.VMEM(tiles, bf16),
        pltpu.VMEM((X, T, 128), jnp.float32),
        pltpu.VMEM((X, T, 128), jnp.float32),
        pltpu.VMEM((Y, X, HU, T), bf16),
        pltpu.VMEM((2, B8, T), bf16),
        pltpu.VMEM((2, n_ep, T), bf16),
        pltpu.SemaphoreType.DMA((2, 2, n_ep)),
        pltpu.SemaphoreType.DMA((2, 3, X)),
        pltpu.SemaphoreType.DMA((2, 2, 2, Y)),
        pltpu.SemaphoreType.DMA((2, X)),
        pltpu.SemaphoreType.DMA((2, 2, 4)),
    ]


def local(
    query_rows,
    key_rows,
    value_rows,
    cum_gate,
    out_weight,
    moe_input,
    moe_gain,
    routes,
    route_weight,
    expert_gate,
    expert_up,
    expert_down,
    shared_gate,
    shared_up,
    shared_down,
):
    n_ep, n_tp = lax.axis_size("ep"), lax.axis_size("tp")
    X = expert_gate.shape[0]
    Y = n_tp // X
    Z = n_ep // 2
    R = query_rows.shape[0]
    CH = 256
    T, D = moe_input.shape
    HU = expert_gate.shape[2]
    vm = pl.BlockSpec(memory_space=pltpu.VMEM)
    step = pl.pallas_call(
        functools.partial(step_kernel, (Z, Y, X, R, CH), STOPS),
        out_shape=(
            jax.ShapeDtypeStruct((R, out_weight.shape[1]), jnp.bfloat16),
            jax.ShapeDtypeStruct((T, out_weight.shape[1]), jnp.bfloat16),
        ),
        in_specs=[vm] * 15,
        out_specs=(vm, vm),
        scratch_shapes=[
            pltpu.VMEM((Z, R // CH, 2, 2 * HEAD, CH), jnp.bfloat16),
            pltpu.VMEM((R, 256), jnp.bfloat16),
            pltpu.VMEM((R, 128), jnp.float32),
            pltpu.VMEM((R, 128), jnp.float32),
            pltpu.VMEM((2, Y, X, R // 4, 128), jnp.bfloat16),
            pltpu.VMEM((n_tp * 128, 256), jnp.bfloat16),
            pltpu.SemaphoreType.DMA((Z, R // CH)),
            pltpu.SemaphoreType.DMA((Z, R // CH)),
            pltpu.SemaphoreType.DMA((Z, R // CH)),
            pltpu.SemaphoreType.DMA((Z, R // CH)),
            pltpu.SemaphoreType.DMA((2, 2, 4)),
            pltpu.SemaphoreType.DMA((2, 2, 4)),
        ]
        + expert_scratch(n_ep, Y, X, T, D, HU, expert_down.shape[1]),
        compiler_params=pltpu.CompilerParams(
            collective_id=0, has_side_effects=True, vmem_limit_bytes=56 * 1024 * 1024
        ),
    )
    return step(
        query_rows.T,
        key_rows.T,
        value_rows.T,
        cum_gate,
        out_weight,
        moe_input,
        moe_gain[None, :],
        routes.T,
        route_weight.T,
        expert_gate.swapaxes(1, 2),
        expert_up.swapaxes(1, 2),
        expert_down,
        shared_gate.T,
        shared_up.T,
        shared_down,
    )


def solution(mesh):
    placed = (
        P("ep", "tp"),
        P("ep", "tp"),
        P("ep", "tp"),
        P("tp", None),
        P(None, "tp"),
        P("ep", None),
        P(),
        P("ep", None),
        P("ep", None),
        P("ep", None, "tp"),
        P("ep", None, "tp"),
        P("ep", None, "tp"),
        P(None, "tp"),
        P(None, "tp"),
        P(None, "tp"),
    )
    return jax.shard_map(
        local, mesh=mesh, in_specs=placed, out_specs=(P("ep", "tp"), P("ep", "tp")), check_vma=False
    )
```

```python
import functools
import jax
import jax.numpy as jnp
from jax import lax
from jax.experimental import pallas as pl
from jax.experimental.pallas import tpu as pltpu
from jax.sharding import PartitionSpec as P

HEAD = 64
TOP = 3
LOG2E = 1.4426950408889634
MESH = pl.DeviceIdType.MESH
STOPS = (2, 5, 10, 11, 14, 17, 20)
neg_fill = -1e30
norm_eps = 1e-06


def in_three(value):
    hi = value.astype(jnp.bfloat16)
    left = value - hi.astype(jnp.float32)
    mid = left.astype(jnp.bfloat16)
    low = (left - mid.astype(jnp.float32)).astype(jnp.bfloat16)
    return hi, mid, low


def step_kernel(dims, stops, *refs):
    qT_ref, kT_ref, vT_ref, cg_ref, w_ref = refs[0:5]
    expert_ins = refs[5:15]
    out_ref, moe_ref = refs[15:17]
    kv, qs, acc, mx, hg, wb, ring_send, ring_recv, pair_send, pair_recv, head_send, head_recv = refs[17:29]
    expert_scratch_refs = refs[29:]
    Z, Y, X, R, CH = dims
    NCH = R // CH
    QT = R // 256
    NU, ND = Z // 2, Z // 2 - 1
    ep = lax.axis_index("ep")
    tp = lax.axis_index("tp")
    z, core = ep // 2, ep % 2
    y, x = tp // X, tp % X
    up = (lax.rem(ep + 2, 2 * Z), tp)
    down = (lax.rem(ep + 2 * Z - 2, 2 * Z), tp)
    partner = (2 * z + 1 - core, tp)

    def x_peer(k):
        return (ep, y * X + lax.rem(x + k, X))

    def y_peer(k):
        return (ep, lax.rem(y + k, Y) * X + x)

    barrier = pltpu.get_barrier_semaphore()
    peers = [x_peer(k) for k in range(1, X)] + [y_peer(k) for k in range(1, Y)]
    for peer in peers:
        pl.semaphore_signal(barrier, inc=1, device_id=peer, device_id_type=MESH)

    def greet(k, carry):
        pl.semaphore_signal(barrier, inc=1, device_id=(lax.rem(ep + k, 2 * Z), tp), device_id_type=MESH)
        return carry

    lax.fori_loop(1, 2 * Z, greet, 0)

    def copy(src, dst, ssem, rsem, dev):
        return pltpu.make_async_remote_copy(
            src_ref=src, dst_ref=dst, send_sem=ssem, recv_sem=rsem,
            device_id=dev, device_id_type=MESH)

    def halves(c, target, ssem, rsem, dev):
        keys = copy(kT_ref.at[:, pl.ds(c * CH, CH)], target.at[0:HEAD], ssem, rsem, dev)
        values = copy(vT_ref.at[:, pl.ds(c * CH, CH)], target.at[HEAD:2 * HEAD], ssem, rsem, dev)
        keys.start()
        values.start()

    def start_first(c, slot, dev):
        halves(c, kv.at[slot, c, 0], ring_send.at[slot, c], ring_recv.at[slot, c], dev)

    def start_first_pair(c):
        halves(c, kv.at[0, c, 1], pair_send.at[0, c], pair_recv.at[0, c], partner)

    def first(c, slot, dev):
        return copy(kv.at[slot, c, 0], kv.at[slot, c, 0], ring_send.at[slot, c], ring_recv.at[slot, c], dev)

    def first_pair(c):
        return copy(kv.at[0, c, 1], kv.at[0, c, 1], pair_send.at[0, c], pair_recv.at[0, c], partner)

    def onward(slot, c, dev):
        return copy(kv.at[slot, c, 0], kv.at[slot + 1, c, 0],
                    ring_send.at[slot + 1, c], ring_recv.at[slot + 1, c], dev)

    def to_pair(slot, c):
        return copy(kv.at[slot, c, 0], kv.at[slot, c, 1],
                    pair_send.at[slot, c], pair_recv.at[slot, c], partner)

    (keep_weights, send_weights, dispatch, send_rows, shared_first, send_shared, shared_second,
     gather_rows, first_products, second_products, combine, finish, drain_experts) = expert_stages(
        (2 * Z, Y, X, expert_ins[0].shape[0]), copy, x_peer, y_peer, expert_ins, moe_ref, expert_scratch_refs)

    dispatch()
    shared_first()
    keep_weights()
    q_all = jnp.transpose(qT_ref[...].astype(jnp.float32)) * (HEAD ** -0.5 * LOG2E)
    q_hi, q_mid, q_lo = in_three(q_all)
    q_one = jnp.where(lax.broadcasted_iota(jnp.int32, (R, HEAD), 1) < 3, 1.0, 0.0).astype(jnp.bfloat16)
    qs[:, 0:128] = jnp.concatenate([q_hi, q_mid], axis=1)
    qs[:, 128:256] = jnp.concatenate([q_lo, q_one], axis=1)
    mx[...] = jnp.full(mx.shape, neg_fill, jnp.float32)
    acc[...] = jnp.zeros(acc.shape, jnp.float32)
    wb[...] = jnp.zeros(wb.shape, jnp.bfloat16)

    def place(h, _):
        part = w_ref[pl.ds(pl.multiple_of(h * HEAD, HEAD), HEAD), :]
        wb[pl.ds(pl.multiple_of(h * 128, 128), HEAD), 0:128] = part
        wb[pl.ds(pl.multiple_of(h * 128 + HEAD, HEAD), HEAD), 128:256] = part
        return 0

    lax.fori_loop(0, w_ref.shape[0] // HEAD, place, 0)

    first_row = pl.multiple_of(ep * R, 128)
    base_gate = cg_ref[:, pl.ds(first_row, 128)][:, 0:1]

    def gate_of(block, c):
        at = pl.multiple_of(block * R + c * CH, 128)
        return (base_gate - cg_ref[:, pl.ds(at, CH)]) * LOG2E

    def score_side(pair, gate):
        hi, mid, lo = in_three(gate)
        row = lax.broadcasted_iota(jnp.int32, (HEAD, CH), 0)
        hi, mid, lo = (piece.astype(jnp.float32) for piece in (hi, mid, lo))
        gates = jnp.where(row == 0, hi, jnp.where(row == 1, mid, jnp.where(row == 2, lo, 0.0)))
        keys = pair[0:HEAD, :]
        return jnp.concatenate([keys, keys, keys, gates.astype(jnp.bfloat16)], axis=0)

    def value_side(pair):
        return jnp.concatenate([jnp.ones((HEAD, CH), jnp.bfloat16), pair[HEAD:2 * HEAD, :]], axis=0)

    def update(i, sides, masked=False):
        rows = slice(i * 256, (i + 1) * 256)
        q = qs[rows, :]
        logits = [jnp.dot(q, keys, preferred_element_type=jnp.float32) for keys, _ in sides]
        if masked:
            qi = lax.broadcasted_iota(jnp.int32, logits[0].shape, 0)
            ki = lax.broadcasted_iota(jnp.int32, logits[0].shape, 1)
            logits[0] = jnp.where(ki <= qi, logits[0], neg_fill)
        tops = [s[:, at:at + 128] for s in logits for at in range(0, CH, 128)]
        top = tops[0]
        for s in tops[1:]:
            top = jnp.maximum(top, s)
        old = mx[rows, :]
        new = jnp.maximum(old, jnp.max(top, axis=1, keepdims=True))
        wide = jnp.concatenate([new] * (CH // 128), axis=1)
        total = acc[rows, :] * jnp.exp2(old - new)
        for s, (_, values) in zip(logits, sides):
            p = jnp.exp2(s - wide).astype(jnp.bfloat16)
            total = total + lax.dot_general(
                p, values, (((1,), (1,)), ((), ())), preferred_element_type=jnp.float32)
        acc[rows, :] = total
        mx[rows, :] = new

    def sides_of(pair, block, c):
        return score_side(pair, gate_of(block, c)), value_side(pair)

    for c in range(NCH):
        side = sides_of(jnp.concatenate([kT_ref[:, c * CH:(c + 1) * CH], vT_ref[:, c * CH:(c + 1) * CH]], axis=0), ep, c)
        for i in range(c, QT):
            update(i, [side], i == c)

    pl.semaphore_wait(barrier, len(peers) + 2 * Z - 1)
    for c in range(NCH):
        @pl.when(z < Z - 1)
        def _():
            start_first(c, 1, up)

        @pl.when(z < ND)
        def _():
            start_first(c, NU + 1, down)

        start_first_pair(c)

    send_rows()
    send_weights()
    send_shared()
    for c in range(NCH):
        first_pair(c).wait_recv()

    @pl.when(core == 1)
    def _():
        for c in range(NCH):
            side = sides_of(kv[0, c, 1], ep - 1, c)
            for i in range(QT):
                update(i, [side])

    def issue(s, c):
        @pl.when(s <= z)
        def _():
            onward(s - 1, c, up).wait_recv()
            to_pair(s, c).start()

            @pl.when(jnp.logical_and(s < NU, z < Z - 1))
            def _():
                onward(s, c, up).start()

        @pl.when(jnp.logical_and(s <= ND, lax.rem(z + s, Z) < ND))
        def _():
            onward(NU + s - 1, c, down).wait_recv()

            @pl.when(s < ND)
            def _():
                onward(NU + s, c, down).start()

            @pl.when(z + s >= Z)
            def _():
                to_pair(NU + s, c).start()

    def attend(slot, chip):
        for c in range(NCH):
            sides = [sides_of(kv[slot, c, 0], 2 * chip + core, c), sides_of(kv[slot, c, 1], 2 * chip + 1 - core, c)]
            for i in range(QT):
                update(i, sides)

    def consume(s):
        @pl.when(s <= z)
        def _():
            for c in range(NCH):
                to_pair(s, c).wait_recv()
            attend(s, z - s)

        @pl.when(jnp.logical_and(s <= ND, z + s >= Z))
        def _():
            for c in range(NCH):
                to_pair(NU + s, c).wait_recv()
            attend(NU + s, z + s - Z)

    steps = NU * NCH

    def step(t, _):
        @pl.when(t < steps)
        def _():
            issue(t // NCH + 1, t % NCH)

        for at, stage in zip(stops, (
            shared_second,
            lambda: gather_rows(0), lambda: first_products(0), lambda: gather_rows(1),
            lambda: second_products(0), lambda: first_products(1), lambda: second_products(1))):
            @pl.when(t == at)
            def _():
                stage()

        @pl.when(jnp.logical_and(t >= NCH, t % NCH == 0))
        def _():
            consume(t // NCH)

        return 0

    lax.fori_loop(0, steps + 1, step, 0)

    quarter, half = R // 4, R // 2
    low = lax.broadcasted_iota(jnp.int32, (quarter, 128), 1) < HEAD

    def finished(at):
        a = acc[at:at + quarter, :]
        return a / pltpu.roll(a, HEAD, 1)

    for h in range(2):
        first_half = pltpu.roll(finished(h * quarter), HEAD, 1)
        second_half = finished(half + h * quarter)
        hg[h, y, x] = jnp.where(low, first_half, second_half).astype(jnp.bfloat16)

    def spread(h, phase, k):
        along_x = (h == 0) == (phase == 0)
        dev = x_peer(k) if along_x else y_peer(k)
        if phase == 0:
            ref = hg.at[h, y, x]
        elif along_x:
            ref = hg.at[h, :, x]
        else:
            ref = hg.at[h, y]
        return copy(ref, ref, head_send.at[h, phase, k], head_recv.at[h, phase, k], dev)

    def spread_in(h, phase, k):
        along_x = (h == 0) == (phase == 0)
        n = X if along_x else Y
        src_x = lax.rem(x + X - k, X)
        src_y = lax.rem(y + Y - k, Y)
        if phase == 0:
            ref = hg.at[h, y, src_x] if along_x else hg.at[h, src_y, x]
        elif along_x:
            ref = hg.at[h, :, src_x]
        else:
            ref = hg.at[h, src_y]
        return copy(ref, ref, head_send.at[h, phase, k], head_recv.at[h, phase, k], partner)

    def count(h, phase):
        return X if (h == 0) == (phase == 0) else Y

    for phase in range(2):
        for h in range(2):
            if phase == 1:
                for k in range(1, count(h, 0)):
                    spread_in(h, 0, k).wait_recv()
            for k in range(1, count(h, phase)):
                spread(h, phase, k).start()
        if phase == 0:
            combine()
        else:
            finish()

    for h in range(2):
        for k in range(1, count(h, 1)):
            spread_in(h, 1, k).wait_recv()
        heads = X * Y
        flat = hg.at[h]
        total = jnp.zeros((quarter, 256), jnp.float32)
        for pair in range(heads // 2):
            a, b = 2 * pair, 2 * pair + 1
            lhs = jnp.concatenate([flat[a // X, a % X], flat[b // X, b % X]], axis=1)
            total = total + jnp.dot(lhs, wb[pair * 256:(pair + 1) * 256, :],
                                    preferred_element_type=jnp.float32)
        out_ref[h * quarter:(h + 1) * quarter, :] = total[:, 0:128].astype(jnp.bfloat16)
        out_ref[half + h * quarter:half + (h + 1) * quarter, :] = total[:, 128:256].astype(jnp.bfloat16)

    for c in range(NCH):
        @pl.when(z < Z - 1)
        def _():
            first(c, 1, up).wait_send()

        @pl.when(z < ND)
        def _():
            first(c, NU + 1, down).wait_send()

        first_pair(c).wait_send()

    def drain(s, _):
        for c in range(NCH):
            @pl.when(s <= z)
            def _():
                to_pair(s, c).wait_send()

                @pl.when(jnp.logical_and(s < NU, z < Z - 1))
                def _():
                    onward(s, c, up).wait_send()

            @pl.when(jnp.logical_and(s <= ND, lax.rem(z + s, Z) < ND))
            def _():
                @pl.when(s < ND)
                def _():
                    onward(NU + s, c, down).wait_send()

                @pl.when(z + s >= Z)
                def _():
                    to_pair(NU + s, c).wait_send()
        return 0

    lax.fori_loop(1, NU + 1, drain, 0)
    drain_experts()
    for phase in range(2):
        for h in range(2):
            for k in range(1, count(h, phase)):
                spread(h, phase, k).wait_send()


def dot_nn(a, b):
    return jnp.dot(a, b, preferred_element_type=jnp.float32)


def dot_nt(a, b):
    return lax.dot_general(a, b, (((1,), (1,)), ((), ())), preferred_element_type=jnp.float32)


def dot_tn(a, b):
    return lax.dot_general(a, b, (((0,), (0,)), ((), ())), preferred_element_type=jnp.float32)


def iota(shape, dim):
    return lax.broadcasted_iota(jnp.int32, shape, dim)


def as_bf16(flags):
    return jnp.where(flags, 1.0, 0.0).astype(jnp.bfloat16)


def expert_stages(dims, copy, x_peer, y_peer, ins, out_ref, scratch):
    n_ep, Y, X, T = dims
    x_in, gain_in, routes_in, share_in, gate_in, up_in, down_in, sgate_in, sup_in, sdown_in = ins
    (normed, ob, rb, fa, gw, uw, dw, ha, ro, cb, ps, pr, sh, mix, mix_end,
     z_sems, w_sems, y_sems, p_sems, s_sems) = scratch
    ep = lax.axis_index("ep")
    tp = lax.axis_index("tp")
    y, x = tp // X, tp % X
    D = normed.shape[1]
    DY = D // Y
    B8 = 8 * n_ep
    quart, nh, bh = n_ep // 4, n_ep // 2, 4 * n_ep
    HU = gate_in.shape[1]

    def ep_peer(k):
        return (lax.rem(ep + k, n_ep), tp)

    def ep_from(k):
        return lax.rem(ep + n_ep - k, n_ep)

    def x_to(k):
        return lax.rem(x + k, X)

    def x_from(k):
        return lax.rem(x + X - k, X)

    def y_from(k):
        return lax.rem(y + Y - k, Y)

    def weight_copies(k, incoming):
        to, place = x_to(k), (x_from(k) if incoming else x)
        rows = pl.ds(pl.multiple_of(place * HU, HU), HU)
        return [
            copy(gate_in.at[to], gw.at[rows], w_sems.at[0, 0, k], w_sems.at[1, 0, k], x_peer(k)),
            copy(up_in.at[to], uw.at[rows], w_sems.at[0, 1, k], w_sems.at[1, 1, k], x_peer(k)),
            copy(down_in.at[to], dw.at[place], w_sems.at[0, 2, k], w_sems.at[1, 2, k], x_peer(k)),
        ]

    def keep_weights():
        rows = pl.ds(pl.multiple_of(x * HU, HU), HU)
        gw[rows, :] = gate_in[x]
        uw[rows, :] = up_in[x]
        dw[x] = down_in[x]

    def send_weights():
        for k in range(1, X):
            for c in weight_copies(k, False):
                c.start()

    def place_of(k):
        return lax.rem(k + quart, n_ep)

    def group_each(g, fn):
        if g == 0:
            each(1, quart, fn)
            each(n_ep - quart, n_ep, fn)
        else:
            each(quart, n_ep - quart, fn)

    def out_copy(k):
        to = lax.rem(ep + k, n_ep)
        return copy(ob.at[to], rb.at[place_of(k)], z_sems.at[0, 0, k], z_sems.at[0, 1, k], ep_peer(k))

    def in_copy(k):
        return copy(ob.at[ep], rb.at[place_of(k)], z_sems.at[0, 0, k], z_sems.at[0, 1, k], ep_peer(k))

    def back_copy(k):
        return copy(ro.at[place_of(k)], cb.at[ep], z_sems.at[1, 0, k], z_sems.at[1, 1, k], (ep_from(k), tp))

    def returned_copy(k):
        return copy(ro.at[0], cb.at[lax.rem(ep + k, n_ep)], z_sems.at[1, 0, k], z_sems.at[1, 1, k], ep_peer(k))

    def each(first, last, fn):
        def body(k, carry):
            fn(k)
            return carry
        lax.fori_loop(first, last, body, 0)

    def row_copy(g, k):
        return copy(fa.at[g, y], fa.at[g, y], y_sems.at[g, 0, 0, k], y_sems.at[g, 0, 1, k], y_peer(k))

    def row_in(g, k):
        return copy(fa.at[g, y], fa.at[g, y_from(k)], y_sems.at[g, 0, 0, k], y_sems.at[g, 0, 1, k], y_peer(k))

    def hid_copy(g, k):
        return copy(ha.at[g, y], ha.at[g, y], y_sems.at[g, 1, 0, k], y_sems.at[g, 1, 1, k], y_peer(k))

    def hid_in(g, k):
        return copy(ha.at[g, y], ha.at[g, y_from(k)], y_sems.at[g, 1, 0, k], y_sems.at[g, 1, 1, k], y_peer(k))

    def part_copy(k):
        return copy(ps.at[x_to(k)], pr.at[x], p_sems.at[0, k], p_sems.at[1, k], x_peer(k))

    def part_in(k):
        return copy(ps.at[x], pr.at[x_from(k)], p_sems.at[0, k], p_sems.at[1, k], x_peer(k))

    def share_x(k):
        return copy(sh.at[y, x], sh.at[y, x], s_sems.at[0, 0, k], s_sems.at[0, 1, k], x_peer(k))

    def share_x_in(k):
        return copy(sh.at[y, x], sh.at[y, x_from(k)], s_sems.at[0, 0, k], s_sems.at[0, 1, k], x_peer(k))

    def share_y(k):
        return copy(sh.at[y], sh.at[y], s_sems.at[1, 0, k], s_sems.at[1, 1, k], y_peer(k))

    def share_y_in(k):
        return copy(sh.at[y], sh.at[y_from(k)], s_sems.at[1, 0, k], s_sems.at[1, 1, k], y_peer(k))

    def pick(wide):
        row = iota((wide.shape[0], 128), 0) % 8
        total = jnp.zeros((wide.shape[0], 128), jnp.float32)
        for c in range(X):
            total = total + jnp.where(row == c, wide[:, c * 128:(c + 1) * 128], 0.0)
        return total

    def to_tiles(value):
        return value.reshape(value.shape[0] // 8, 8, 128).astype(jnp.bfloat16)

    def from_tiles(tiles):
        return tiles.astype(jnp.float32).reshape(tiles.shape[0] * 8, 128).astype(jnp.bfloat16)

    def ninth(tile, c):
        n = tile.shape[0] // 8
        chosen = as_bf16(iota((n, 8 * n), 1) == 8 * iota((n, 8 * n), 0) + c)
        return dot_nn(chosen, tile)

    def spread_rows(value):
        n = value.shape[0]
        expand = as_bf16(iota((8 * n, n), 0) // 8 == iota((8 * n, n), 1))
        return dot_nn(expand, value)

    def dispatch():
        rows = x_in[...].astype(jnp.float32)
        mean = jnp.mean(rows * rows, axis=1, keepdims=True)
        normed[...] = (rows * lax.rsqrt(mean + norm_eps) * gain_in[...]).astype(jnp.bfloat16)
        named = iota((n_ep, T), 0) * X + x
        hit = jnp.zeros((n_ep, T), jnp.float32)
        weight = jnp.zeros((n_ep, T), jnp.float32)
        for j in range(TOP):
            same = named == routes_in[j:j + 1, :]
            hit = hit + jnp.where(same, 1.0, 0.0)
            weight = weight + jnp.where(same, share_in[j:j + 1, :], 0.0)
        before = as_bf16(iota((T, T), 0) < iota((T, T), 1))
        rank = jnp.where(hit > 0.0, dot_nn(hit.astype(jnp.bfloat16), before), -1.0)
        place = spread_rows(rank.astype(jnp.bfloat16))
        mine = normed[:, pl.ds(pl.multiple_of(y * DY, 128), DY)]
        slot = (iota((B8, T), 0) % 8).astype(jnp.float32)
        main = dot_nn(as_bf16(place == slot), mine)
        last = pick(dot_nn(as_bf16(place == 8.0), mine))
        for c in range(X):
            ob[:, c] = to_tiles(main[:, c * 128:(c + 1) * 128])
        ob[:, X] = to_tiles(last)
        rb[quart] = ob[ep]
        high = weight.astype(jnp.bfloat16)
        low = (weight - high.astype(jnp.float32)).astype(jnp.bfloat16)
        for n, piece in enumerate((high, low)):
            mix[n] = jnp.where(place == slot, spread_rows(piece), 0.0).astype(jnp.bfloat16)
            mix_end[n] = jnp.where(rank == 8.0, piece.astype(jnp.float32), 0.0).astype(jnp.bfloat16)

    def send_rows():
        for g in range(2):
            group_each(g, lambda k: out_copy(k).start())

    def shared_first():
        gate = dot_nt(sgate_in[...], normed[...])
        up = dot_nt(sup_in[...], normed[...])
        sh[y, x] = (gate / (1.0 + jnp.exp(-gate)) * up).astype(jnp.bfloat16)

    def send_shared():
        for k in range(1, X):
            share_x(k).start()

    def shared_second():
        for k in range(1, X):
            share_x_in(k).wait_recv()
        for k in range(1, Y):
            share_y(k).start()

    def gather_rows(g):
        group_each(g, lambda k: in_copy(k).wait_recv())
        span = slice(g * nh, (g + 1) * nh)
        tile = from_tiles(rb[span, X])
        for c in range(X):
            fa[g, y, 0:bh, c * 128:(c + 1) * 128] = from_tiles(rb[span, c])
            fa[g, y, bh:bh + nh, c * 128:(c + 1) * 128] = ninth(tile, c).astype(jnp.bfloat16)
        for k in range(1, Y):
            row_copy(g, k).start()

    def first_products(g):
        if g == 0:
            for k in range(1, X):
                for c in weight_copies(k, True):
                    c.wait_recv()
        for k in range(1, Y):
            row_in(g, k).wait_recv()
        gate = jnp.zeros((bh + nh, X * HU), jnp.float32)
        up = jnp.zeros((bh + nh, X * HU), jnp.float32)
        for part in range(Y):
            piece = fa[g, part]
            gate = gate + dot_nt(piece, gw[:, part * DY:(part + 1) * DY])
            up = up + dot_nt(piece, uw[:, part * DY:(part + 1) * DY])
        ha[g, y] = (gate / (1.0 + jnp.exp(-gate)) * up).astype(jnp.bfloat16)
        for k in range(1, Y):
            hid_copy(g, k).start()

    def second_products(g):
        for k in range(1, Y):
            hid_in(g, k).wait_recv()
        hidden = jnp.concatenate([ha[g, part] for part in range(Y)], axis=1)
        span = slice(g * nh, (g + 1) * nh)
        ends = []
        for c in range(X):
            result = dot_nn(hidden, dw[c])
            ro[span, c] = to_tiles(result[0:bh])
            ends.append(result[bh:bh + nh].astype(jnp.bfloat16))
        ro[span, X] = to_tiles(pick(spread_rows(jnp.concatenate(ends, axis=1))))
        group_each(g, lambda k: back_copy(k).start())
        if g == 0:
            cb[ep] = ro[quart]

    def combine():
        each(1, n_ep, lambda k: returned_copy(k).wait_recv())
        main = jnp.concatenate([from_tiles(cb[:, c]) for c in range(X)], axis=1)
        tile = from_tiles(cb[:, X])
        last = jnp.concatenate([ninth(tile, c).astype(jnp.bfloat16) for c in range(X)], axis=1)
        total = jnp.zeros((T, DY), jnp.float32)
        for n in range(2):
            total = total + dot_tn(mix[n], main) + dot_tn(mix_end[n], last)
        for c in range(X):
            ps[c] = total[:, c * 128:(c + 1) * 128]
        for k in range(1, X):
            part_copy(k).start()

    def finish():
        for k in range(1, Y):
            share_y_in(k).wait_recv()
        hidden = jnp.concatenate([sh[a, b] for a in range(Y) for b in range(X)], axis=0)
        total = dot_tn(hidden, sdown_in[...])
        for k in range(1, X):
            part_in(k).wait_recv()
        total = total + ps[x]
        for k in range(1, X):
            total = total + pr[x_from(k)]
        out_ref[...] = total.astype(jnp.bfloat16)

    def drain():
        each(1, n_ep, lambda k: out_copy(k).wait_send())
        each(1, n_ep, lambda k: back_copy(k).wait_send())
        for k in range(1, X):
            for c in weight_copies(k, False):
                c.wait_send()
            share_x(k).wait_send()
            part_copy(k).wait_send()
        for k in range(1, Y):
            share_y(k).wait_send()
            for g in range(2):
                row_copy(g, k).wait_send()
                hid_copy(g, k).wait_send()

    return (keep_weights, send_weights, dispatch, send_rows, shared_first, send_shared, shared_second,
            gather_rows, first_products, second_products, combine, finish, drain)


def expert_scratch(n_ep, Y, X, T, D, HU, FF):
    B8 = 8 * n_ep
    tiles = (n_ep, X + 1, 8, 128)
    bf16 = jnp.bfloat16
    return [
        pltpu.VMEM((T, D), bf16),
        pltpu.VMEM(tiles, bf16),
        pltpu.VMEM(tiles, bf16),
        pltpu.VMEM((2, Y, (B8 + n_ep) // 2, D // Y), bf16),
        pltpu.VMEM((X * HU, D), bf16),
        pltpu.VMEM((X * HU, D), bf16),
        pltpu.VMEM((X, FF, 128), bf16),
        pltpu.VMEM((2, Y, (B8 + n_ep) // 2, X * HU), bf16),
        pltpu.VMEM(tiles, bf16),
        pltpu.VMEM(tiles, bf16),
        pltpu.VMEM((X, T, 128), jnp.float32),
        pltpu.VMEM((X, T, 128), jnp.float32),
        pltpu.VMEM((Y, X, HU, T), bf16),
        pltpu.VMEM((2, B8, T), bf16),
        pltpu.VMEM((2, n_ep, T), bf16),
        pltpu.SemaphoreType.DMA((2, 2, n_ep)),
        pltpu.SemaphoreType.DMA((2, 3, X)),
        pltpu.SemaphoreType.DMA((2, 2, 2, Y)),
        pltpu.SemaphoreType.DMA((2, X)),
        pltpu.SemaphoreType.DMA((2, 2, 4)),
    ]


def local(
    query_rows,
    key_rows,
    value_rows,
    cum_gate,
    out_weight,
    moe_input,
    moe_gain,
    routes,
    route_weight,
    expert_gate,
    expert_up,
    expert_down,
    shared_gate,
    shared_up,
    shared_down,
):
    n_ep, n_tp = lax.axis_size("ep"), lax.axis_size("tp")
    X = expert_gate.shape[0]
    Y = n_tp // X
    Z = n_ep // 2
    R = query_rows.shape[0]
    CH = 256
    T, D = moe_input.shape
    HU = expert_gate.shape[2]
    vm = pl.BlockSpec(memory_space=pltpu.VMEM)
    step = pl.pallas_call(
        functools.partial(step_kernel, (Z, Y, X, R, CH), STOPS),
        out_shape=(
            jax.ShapeDtypeStruct((R, out_weight.shape[1]), jnp.bfloat16),
            jax.ShapeDtypeStruct((T, out_weight.shape[1]), jnp.bfloat16),
        ),
        in_specs=[vm] * 15,
        out_specs=(vm, vm),
        scratch_shapes=[
            pltpu.VMEM((Z, R // CH, 2, 2 * HEAD, CH), jnp.bfloat16),
            pltpu.VMEM((R, 256), jnp.bfloat16),
            pltpu.VMEM((R, 128), jnp.float32),
            pltpu.VMEM((R, 128), jnp.float32),
            pltpu.VMEM((2, Y, X, R // 4, 128), jnp.bfloat16),
            pltpu.VMEM((n_tp * 128, 256), jnp.bfloat16),
            pltpu.SemaphoreType.DMA((Z, R // CH)),
            pltpu.SemaphoreType.DMA((Z, R // CH)),
            pltpu.SemaphoreType.DMA((Z, R // CH)),
            pltpu.SemaphoreType.DMA((Z, R // CH)),
            pltpu.SemaphoreType.DMA((2, 2, 4)),
            pltpu.SemaphoreType.DMA((2, 2, 4)),
        ]
        + expert_scratch(n_ep, Y, X, T, D, HU, expert_down.shape[1]),
        compiler_params=pltpu.CompilerParams(
            collective_id=0, has_side_effects=True, vmem_limit_bytes=56 * 1024 * 1024
        ),
    )
    return step(
        query_rows.T,
        key_rows.T,
        value_rows.T,
        cum_gate,
        out_weight,
        moe_input,
        moe_gain[None, :],
        routes.T,
        route_weight.T,
        expert_gate.swapaxes(1, 2),
        expert_up.swapaxes(1, 2),
        expert_down,
        shared_gate.T,
        shared_up.T,
        shared_down,
    )


def solution(mesh):
    placed = (
        P("ep", "tp"),
        P("ep", "tp"),
        P("ep", "tp"),
        P("tp", None),
        P(None, "tp"),
        P("ep", None),
        P(),
        P("ep", None),
        P("ep", None),
        P("ep", None, "tp"),
        P("ep", None, "tp"),
        P("ep", None, "tp"),
        P(None, "tp"),
        P(None, "tp"),
        P(None, "tp"),
    )
    return jax.shard_map(
        local, mesh=mesh, in_specs=placed, out_specs=(P("ep", "tp"), P("ep", "tp")), check_vma=False
    )
```
